256 devices in a mesh: grp: 2 (over z), st: 16 (over y, core), tp: 8 (over x).
Axes of the slice: x: 8, y: 8, z: 2, core: 2. Of those that a mesh axis runs over, the one named last changes fastest.
The devices are a block of a 8x8x16 slice.
Arguments:
- tokens: bfloat16 [32768, 2048], P(('grp', 'st')), parts along dimension 0, may hold values from -6 to 6
- w_query: bfloat16 [2048, 512], P(None, 'tp'), may hold values from -0.125 to 0.125
- w_key: bfloat16 [2048, 512], P(None, 'tp'), may hold values from -0.125 to 0.125
- w_value: bfloat16 [2048, 1024], P(None, 'tp'), may hold values from -0.125 to 0.125
- w_decay: bfloat16 [2048, 512], P(None, 'tp'), may hold values from -0.125 to 0.125
- decay_rate: float32 [512], P('tp'), may hold values from 0.0002 to 0.04
- block_scale: float32 [256], P(('grp', 'st')), parts along dimension 0, may hold values from 0.5 to 2
- w_rquery: bfloat16 [2048, 1024], P(None, 'tp'), may hold values from -0.125 to 0.125
- w_gate: bfloat16 [2048, 1024], P(None, 'tp'), may hold values from -0.125 to 0.125
- w_rkey: bfloat16 [2048, 1024], P(None, 'tp'), may hold values from -0.125 to 0.125
- w_rvalue: bfloat16 [2048, 1024], P(None, 'tp'), may hold values from -3 to 3
- query_gain: float32 [128], replicated, may hold values from 0.1 to 1.9
- key_gain: float32 [128], replicated, may hold values from 0.1 to 1.9
- out_gain: float32 [1024], P('tp'), may hold values from 0.1 to 1.9
- store: bfloat16 [384, 128, 2048], P(('grp', 'st')), parts along dimension 0, may hold values from -6 to 6
- passage_ids: int32 [256, 4], P(('grp', 'st')), parts along dimension 0, may hold values from 0 to 191, as said below
Outputs:
- output: bfloat16 [32768, 1024], P(('grp', 'st'), 'tp'), parts along dimension 0
The draws below stay inside these ranges and needn't reach their ends.
There are 2 independent parts, one for each index of `grp`. The reference program is written for one: setup_inputs(seed, part) draws one part's arguments, and reference() takes and returns one part's arrays. A program takes and returns all parts, laid end to end along the dimension named above; an argument that names none is the same for every part. Nothing has to cross between parts.
Inputs may be any that keep to these rules, and one draw needn't show every extreme that they name: `passage_ids`: passage p is held by index p // 12 of st. The 32 reads of the blocks of one index of st name passages of exactly 16 indices of st, exactly 2 reads of each; among them are always the index before its own and the index half the axis away.
All inputs are finite; a program needn't handle non-finite values.
Results may differ from the reference program's by a relative error of at most 0.0044.
Values may be sent and summed in bfloat16 or wider, within the bound.
No kernel may reach another device: no remote copies, remote signals or barrier semaphores. Data moves between devices by JAX's collectives and lax.ppermute only.
A program may use at most 128 MiB of HBM per device.

```python
import math
import jax
import jax.numpy as jnp
from jax import lax

D = 2048
HEADS = 8
DK = 64
DV = 128
LEN = 1024
BLK = 128
NPASS = 4
PLEN = 128
PASS_DEV = 12
TOKENS = 16384
BLOCKS = 8
REQS = 32
OWNERS = 16
MOST = 2
PASSAGES = 192
N_ST = 16


def draw_passage_ids(key, part):

    def one_index(index_key, device_index):
        key_pool, key_order, key_first, key_second = jax.random.split(index_key, 4)
        offset_pool = jax.random.permutation(key_pool, N_ST - 2).astype(jnp.int32)
        offset_pool = jnp.where(offset_pool < N_ST // 2, offset_pool, offset_pool + 1)
        forced = jnp.array([N_ST - 1, N_ST // 2], jnp.int32)
        offsets = jnp.concatenate([forced, offset_pool])[:OWNERS]
        request_order = jax.random.permutation(key_order, REQS).astype(jnp.int32)
        owner_index = (device_index + offsets[request_order // MOST]) % N_ST
        draw_first = jax.random.randint(key_first, (REQS,), 0, PASS_DEV, dtype=jnp.int32)
        draw_second = jax.random.randint(key_second, (REQS,), 0, PASS_DEV, dtype=jnp.int32)
        local_row = jnp.minimum(draw_first, draw_second)
        return (owner_index * PASS_DEV + local_row).reshape(BLOCKS, NPASS)
    index_keys = jax.random.split(key, N_ST)
    drawn = jax.vmap(one_index)(index_keys, jnp.arange(N_ST, dtype=jnp.int32))
    return drawn.reshape(N_ST * BLOCKS, NPASS).astype(jnp.int32)


def draw_decay_rate(key, part):
    key_kind, key_slow, key_fast = jax.random.split(key, 3)
    fast_cut = 8
    is_fast = jax.random.randint(key_kind, (HEADS,), 0, 16) < fast_cut
    slow_rate = jnp.exp(jax.random.uniform(key_slow, (HEADS, DK), jnp.float32, jnp.log(0.0002), jnp.log(0.0008)))
    fast_rate = jnp.exp(jax.random.uniform(key_fast, (HEADS, DK), jnp.float32, jnp.log(0.015), jnp.log(0.04)))
    return jnp.where(is_fast[:, None], fast_rate, slow_rate).reshape(HEADS * DK).astype(jnp.float32)


def level_of(stream_key, dims, cuts, smallest, largest):
    factor_of, own = 1.0, jax.random.fold_in(stream_key, 6)
    for position, blocks in cuts:
        steps = jnp.exp(jax.random.uniform(jax.random.fold_in(own, position), (blocks,), jnp.float32, smallest / len(cuts), largest / len(cuts)))
        factor_of = factor_of * jnp.repeat(steps, dims[position] // blocks).reshape([-1 if axis == position else 1 for axis in range(len(dims))])
    return factor_of


def normal_values(rng, shape, deviation, limit, cuts=(), held_as=jnp.bfloat16):
    entries = deviation * jax.random.normal(rng, shape, jnp.float32)
    if cuts:
        entries = entries * level_of(rng, shape, cuts, -0.22, 0.18)
    return jnp.clip(entries, -limit, limit).astype(held_as)


def setup_inputs(seed: int = 0, part: int = 0) -> dict:
    streams_of = jax.random.split(jax.random.key(seed), 17)
    part_keys = jax.random.split(jax.random.fold_in(streams_of[16], part), 17)
    tokens = normal_values(part_keys[0], (TOKENS, D), 1.0, 6.0, ((0, 16),))
    w_query = normal_values(streams_of[1], (D, HEADS * DK), D ** -0.5, 0.125, ((1, 8),))
    w_key = normal_values(streams_of[2], (D, HEADS * DK), D ** -0.5, 0.125, ((1, 8),))
    w_value = normal_values(streams_of[3], (D, HEADS * DV), D ** -0.5, 0.125, ((1, 8),))
    w_decay = normal_values(streams_of[4], (D, HEADS * DK), D ** -0.5, 0.125, ((1, 8),))
    decay_rate = draw_decay_rate(jax.random.fold_in(streams_of[16], 71), part)
    block_scale = jnp.clip(jnp.exp(math.log(2.0) - 1.3862944 * jax.random.uniform(part_keys[6], (TOKENS // BLK,), jnp.float32) ** level_of(part_keys[6], (TOKENS // BLK,), ((0, 16),), -0.2, 0.2)), 0.5, 2.0)
    w_rquery = normal_values(streams_of[7], (D, HEADS * DV), D ** -0.5, 0.125, ((1, 8),))
    w_gate = normal_values(streams_of[8], (D, HEADS * DV), D ** -0.5, 0.125, ((1, 8),))
    w_rkey = normal_values(streams_of[9], (D, HEADS * DV), D ** -0.5, 0.125, ((1, 8),))
    w_rvalue = normal_values(streams_of[10], (D, HEADS * DV), (max(1, D // 512)) ** -0.5, 3.0, ((1, 8),))
    query_gain = jnp.clip(1.0 + 0.18 * jax.random.normal(streams_of[11], (DV,), jnp.float32), 0.1, 1.9)
    key_gain = jnp.clip(1.0 + 0.18 * jax.random.normal(streams_of[12], (DV,), jnp.float32), 0.1, 1.9)
    out_gain = jnp.clip(1.0 + 0.18 * jax.random.normal(streams_of[13], (HEADS * DV,), jnp.float32), 0.1, 1.9)
    store = normal_values(part_keys[14], (PASSAGES, PLEN, D), 1.0, 6.0, ((0, 16),))
    passage_ids = draw_passage_ids(jax.random.fold_in(jax.random.fold_in(streams_of[16], part), 71), part)
    return dict(tokens=tokens, w_query=w_query, w_key=w_key, w_value=w_value, w_decay=w_decay, decay_rate=decay_rate, block_scale=block_scale, w_rquery=w_rquery, w_gate=w_gate, w_rkey=w_rkey, w_rvalue=w_rvalue, query_gain=query_gain, key_gain=key_gain, out_gain=out_gain, store=store, passage_ids=passage_ids)


EPS = 1e-06
PRECISE = lax.Precision.HIGHEST

def head_norm(values, gain_row):
    return values * lax.rsqrt(lax.optimization_barrier(jnp.mean(values * values, axis=-1, keepdims=True)) + EPS) * gain_row

def gla_blocks(gla_query, gla_key, gla_value, log_decay):
    head_dim = gla_query.shape[-1]
    block_len = gla_query.shape[1]
    cumulative = jnp.cumsum(log_decay, axis=1)
    query_dec = gla_query * head_dim ** (-0.5) * jnp.exp(cumulative)
    key_dec = gla_key * jnp.exp(-cumulative)
    causal_mask = jnp.arange(block_len)[:, None] >= jnp.arange(block_len)[None, :]
    scores = jnp.einsum('nihd,njhd->nhij', query_dec, key_dec, precision=PRECISE)
    scores = jnp.where(causal_mask, scores, 0.0)
    within = jnp.einsum('nhij,njhv->nihv', scores, gla_value, precision=PRECISE)
    block_total = cumulative[:, -1:]
    update = jnp.einsum('njhd,njhv->nhdv', gla_key * jnp.exp(block_total - cumulative), gla_value, precision=PRECISE)
    carry_decay = jnp.exp(block_total[:, 0])

    def advance(carry_state, block_item):
        query_part, state_delta, factor = block_item
        result = jnp.einsum('ihd,hdv->ihv', query_part, carry_state, precision=PRECISE)
        return (factor[..., None] * carry_state + state_delta, result)
    start_state = jnp.zeros((gla_query.shape[2], head_dim, gla_value.shape[-1]), jnp.float32)
    _, carried = lax.scan(advance, start_state, (query_dec, update, carry_decay))
    return within + carried

def reference(tokens, w_query, w_key, w_value, w_decay, decay_rate, block_scale, w_rquery, w_gate, w_rkey, w_rvalue, query_gain, key_gain, out_gain, store, passage_ids):
    seq_count = TOKENS // LEN
    gla_q = jnp.dot(tokens, w_query, preferred_element_type=jnp.float32)
    gla_k = jnp.dot(tokens, w_key, preferred_element_type=jnp.float32)
    gla_v = jnp.dot(tokens, w_value, preferred_element_type=jnp.float32)
    decay_pre = jnp.dot(tokens, w_decay, preferred_element_type=jnp.float32)
    log_decay = -2.0 * decay_rate[None, :] * jax.nn.sigmoid(decay_pre) * jnp.repeat(block_scale, BLK)[:, None]

    def shaped(values, width):
        return values.reshape(seq_count, LEN // BLK, BLK, HEADS, width)

    def one_sequence(seq_item):
        return gla_blocks(*seq_item)
    gla_out = lax.map(one_sequence, (shaped(gla_q, DK), shaped(gla_k, DK), shaped(gla_v, DV), shaped(log_decay, DK)))
    gla_out = gla_out.reshape(TOKENS, HEADS * DV)
    read_query = jnp.dot(tokens, w_rquery, preferred_element_type=jnp.float32).reshape(TOKENS, HEADS, DV)
    read_query = head_norm(read_query, query_gain).astype(jnp.bfloat16)
    read_query = read_query.reshape(TOKENS // BLK, BLK, HEADS, DV)

    def one_block(block_item):
        block_query, block_ids = block_item
        held_rows = jnp.take(store, block_ids.astype(jnp.int32), axis=0).reshape(NPASS * PLEN, D)
        passage_keys = jnp.dot(held_rows, w_rkey, preferred_element_type=jnp.float32).astype(jnp.bfloat16)
        passage_values = jnp.dot(held_rows, w_rvalue, preferred_element_type=jnp.float32).astype(jnp.bfloat16)
        key_normed = head_norm(passage_keys.astype(jnp.float32).reshape(NPASS * PLEN, HEADS, DV), key_gain).astype(jnp.bfloat16)
        scores = jnp.einsum('qhd,khd->hqk', block_query.astype(jnp.float32), key_normed.astype(jnp.float32), precision=PRECISE) * DV ** (-0.5)
        expd = jnp.exp(scores)
        read_weight = (expd / lax.optimization_barrier(jnp.sum(expd, axis=-1, keepdims=True))).astype(jnp.bfloat16)
        value_rows = passage_values.astype(jnp.float32).reshape(NPASS * PLEN, HEADS, DV)
        return jnp.einsum('hqk,khd->qhd', read_weight.astype(jnp.float32), value_rows, precision=PRECISE)
    retrieved = lax.map(one_block, (read_query, passage_ids)).reshape(TOKENS, HEADS * DV)
    gate_value = jax.nn.sigmoid(jnp.dot(tokens, w_gate, preferred_element_type=jnp.float32))
    combined = gla_out + gate_value * retrieved
    square_mean = lax.optimization_barrier(jnp.mean(combined * combined, axis=1, keepdims=True))
    return (combined * lax.rsqrt(square_mean + EPS) * out_gain[None, :]).astype(jnp.bfloat16)
```

```python
import functools

import jax
import jax.numpy as jnp
from jax import lax
from jax.experimental import pallas as pl
from jax.experimental.pallas import tpu as pltpu
from jax.sharding import PartitionSpec as P

HEADS = 8
DK = 64
DV = 128
BLK = 128
NPASS = 4
EPS = 1e-06
PRECISE = lax.Precision.HIGHEST
F32 = jnp.float32
BF16 = jnp.bfloat16


def nt(a, b, precision=None):
    return lax.dot_general(a, b, (((1,), (1,)), ((), ())), precision=precision, preferred_element_type=F32)


def head_norm(values, gain_row):
    return values * lax.rsqrt(jnp.mean(values * values, axis=-1, keepdims=True) + EPS) * gain_row


def requests_kernel(here, most, ids_ref, wanted_ref, slot_ref, count_ref):
    owners = count_ref.shape[0]

    def clear(i, _):
        count_ref[i] = 0
        return 0

    lax.fori_loop(0, owners, clear, 0)
    blocks, passes = ids_ref.shape

    def one(i, _):
        wanted = ids_ref[i // passes, i % passes]
        owner = jnp.clip(lax.div(wanted, jnp.int32(here)), 0, owners - 1)
        rank = jnp.minimum(count_ref[owner], most - 1)
        count_ref[owner] = rank + 1
        wanted_ref[owner, rank] = wanted - owner * here
        slot_ref[i] = owner * most + rank
        return 0

    lax.fori_loop(0, blocks * passes, one, 0)


def passages_kernel(store_ref, wk_ref, wv_ref, gain_ref, out_ref, weight_ref):
    @pl.when(pl.program_id(0) == 0)
    def _():
        weight_ref[:, :DV] = wk_ref[...]
        weight_ref[:, DV:] = wv_ref[...]

    count, rows, width = store_ref.shape
    made = jnp.dot(store_ref[...].reshape(count * rows, width), weight_ref[...], preferred_element_type=F32)
    made = made.astype(BF16)
    keys = head_norm(made[:, :DV].astype(F32), gain_ref[...]).astype(BF16)
    out_ref[:, :, :DV] = keys.reshape(count, rows, DV)
    out_ref[:, :, DV:] = made[:, DV:].reshape(count, rows, DV)


def pack_kernel(wanted_ref, made_ref, out_ref, sems):
    held = made_ref.shape[0]
    most = wanted_ref.shape[1]

    def copy(i):
        row = jnp.clip(wanted_ref[i // most, i % most], 0, held - 1)
        return pltpu.make_async_copy(made_ref.at[row], out_ref.at[i], sems.at[i])

    count = out_ref.shape[0]
    for i in range(count):
        copy(i).start()
    for i in range(count):
        copy(i).wait()


def tokens_kernel(
    after_ref,
    scale_ref,
    tok_ref,
    wq_ref,
    wk_ref,
    wv_ref,
    wd_ref,
    wr_ref,
    wg_ref,
    rate_ref,
    qgain_ref,
    gla_ref,
    gate_ref,
    rq_ref,
    state_ref,
):
    step = pl.program_id(0)

    @pl.when(step == 0)
    def _():
        state_ref[...] = jnp.zeros_like(state_ref)

    tokens = tok_ref[...]
    rows = tokens.shape[0]

    def times(w_ref):
        return jnp.dot(tokens, w_ref[...], preferred_element_type=F32)

    query = times(wq_ref)
    key = times(wk_ref)
    value = times(wv_ref)
    decay = times(wd_ref)
    rq_ref[...] = head_norm(times(wr_ref), qgain_ref[...]).astype(BF16)
    gate_ref[...] = jax.nn.sigmoid(times(wg_ref))
    row_id = lax.broadcasted_iota(jnp.int32, (BLK, BLK), 0)
    col_id = lax.broadcasted_iota(jnp.int32, (BLK, BLK), 1)
    causal = row_id >= col_id
    lower = causal.astype(F32)
    for b in range(rows // BLK):
        at = slice(b * BLK, (b + 1) * BLK)
        log_decay = -2.0 * rate_ref[...] * jax.nn.sigmoid(decay[at]) * scale_ref[step * (rows // BLK) + b]
        total = jnp.dot(lower, log_decay, precision=PRECISE, preferred_element_type=F32)
        last = total[BLK - 1 : BLK]
        q_dec = query[at] * DK ** (-0.5) * jnp.exp(total)
        k_dec = key[at] * jnp.exp(-total)
        scores = jnp.where(causal, nt(q_dec, k_dec, PRECISE), 0.0)
        within = jnp.dot(scores, value[at], precision=PRECISE, preferred_element_type=F32)
        gla_ref[at] = within + nt(q_dec, state_ref[...], PRECISE)
        update = lax.dot_general(
            value[at],
            key[at] * jnp.exp(last - total),
            (((0,), (0,)), ((), ())),
            precision=PRECISE,
            preferred_element_type=F32,
        )
        state_ref[...] = state_ref[...] * jnp.exp(last) + update


def reads_kernel(slot_ref, got_ref, rq_ref, gla_ref, gate_ref, out_ref, square_ref, held_ref, sems):
    step = pl.program_id(0)
    count = got_ref.shape[0]

    def copy(i):
        slot = jnp.clip(slot_ref[i], 0, count - 1)
        return pltpu.make_async_copy(got_ref.at[slot], held_ref.at[i], sems.at[i])

    @pl.when(step == 0)
    def _():
        for i in range(count):
            copy(i).start()

    for j in range(NPASS):
        copy(step * NPASS + j).wait()
    query = rq_ref[...]
    first = step * NPASS
    rows = held_ref.shape[1]
    parts = []
    for j in range(NPASS):
        parts.append(jnp.exp(nt(query, held_ref[first + j, :, :DV]) * DV ** (-0.5)))
    bottom = sum(jnp.sum(p, axis=-1, keepdims=True) for p in parts)
    read = jnp.zeros((query.shape[0], DV), F32)
    for j in range(NPASS):
        weight = (parts[j] / bottom).astype(BF16)
        read += jnp.dot(weight, held_ref[first + j, :, DV:], preferred_element_type=F32)
    combined = gla_ref[...] + gate_ref[...] * read
    out_ref[...] = combined
    sums = nt(jnp.ones((8, DV), F32), combined * combined, PRECISE)
    square_ref[...] = jnp.broadcast_to(sums[0:1].reshape(1, 1, 1, BLK), square_ref.shape)


def scale_kernel(square_ref, combined_ref, gain_ref, out_ref):
    total = jnp.sum(square_ref[...], axis=0)[:, 0, :]
    scale = lax.rsqrt(total / (HEADS * DV) + EPS)
    columns = jnp.transpose(scale)
    for b in range(total.shape[0]):
        at = slice(b * BLK, (b + 1) * BLK)
        out_ref[at] = (combined_ref[at] * columns[:, b : b + 1] * gain_ref[...]).astype(BF16)


VMEM = pl.BlockSpec(memory_space=pltpu.VMEM)
SMEM = pl.BlockSpec(memory_space=pltpu.SMEM)
ANY = pl.BlockSpec(memory_space=pl.ANY)


def whole(shape):
    return pl.BlockSpec(shape, lambda i: (0,) * len(shape))


def on_device(
    tokens,
    w_query,
    w_key,
    w_value,
    w_decay,
    decay_rate,
    block_scale,
    w_rquery,
    w_gate,
    w_rkey,
    w_rvalue,
    query_gain,
    key_gain,
    out_gain,
    store,
    passage_ids,
):
    length, width = tokens.shape
    blocks = length // BLK
    held, plen, _ = store.shape
    st_size = lax.axis_size("st")
    tp_size = lax.axis_size("tp")
    requests = passage_ids.shape[0] * passage_ids.shape[1]
    owners = min(st_size, requests // 2)
    most = requests // owners
    slots = st_size * most

    wanted, slot_index = pl.pallas_call(
        functools.partial(requests_kernel, held, most),
        out_shape=(
            jax.ShapeDtypeStruct((st_size, most), jnp.int32),
            jax.ShapeDtypeStruct((requests,), jnp.int32),
        ),
        in_specs=[SMEM],
        out_specs=(SMEM, SMEM),
        scratch_shapes=[pltpu.SMEM((st_size,), jnp.int32)],
        name="requests",
    )(passage_ids)
    incoming = lax.all_to_all(wanted, "st", split_axis=0, concat_axis=0, tiled=True)

    step_passages = 2
    made = pl.pallas_call(
        passages_kernel,
        grid=(held // step_passages,),
        out_shape=jax.ShapeDtypeStruct((held, plen, 2 * DV), BF16),
        in_specs=[
            pl.BlockSpec((step_passages, plen, width), lambda i: (i, 0, 0)),
            whole((width, DV)),
            whole((width, DV)),
            whole((1, DV)),
        ],
        out_specs=pl.BlockSpec((step_passages, plen, 2 * DV), lambda i: (i, 0, 0)),
        scratch_shapes=[pltpu.VMEM((width, 2 * DV), BF16)],
        cost_estimate=pl.CostEstimate(
            flops=2 * held * plen * width * 2 * DV,
            bytes_accessed=2 * held * plen * (width + 2 * DV),
            transcendentals=0,
        ),
        name="passages",
    )(store, w_rkey, w_rvalue, key_gain.reshape(1, DV))

    packed = pl.pallas_call(
        pack_kernel,
        out_shape=jax.ShapeDtypeStruct((slots, plen, 2 * DV), BF16),
        in_specs=[SMEM, VMEM],
        out_specs=ANY,
        scratch_shapes=[pltpu.SemaphoreType.DMA((slots,))],
        name="pack",
    )(incoming, made)
    got = lax.all_to_all(packed, "st", split_axis=0, concat_axis=0, tiled=True)

    rows = 2 * BLK
    gla, gate, read_query = pl.pallas_call(
        tokens_kernel,
        grid=(length // rows,),
        out_shape=(
            jax.ShapeDtypeStruct((length, DV), F32),
            jax.ShapeDtypeStruct((length, DV), F32),
            jax.ShapeDtypeStruct((length, DV), BF16),
        ),
        in_specs=[
            ANY,
            SMEM,
            pl.BlockSpec((rows, width), lambda i: (i, 0)),
            whole((width, DK)),
            whole((width, DK)),
            whole((width, DV)),
            whole((width, DK)),
            whole((width, DV)),
            whole((width, DV)),
            whole((1, DK)),
            whole((1, DV)),
        ],
        out_specs=(
            pl.BlockSpec((rows, DV), lambda i: (i, 0)),
            pl.BlockSpec((rows, DV), lambda i: (i, 0)),
            pl.BlockSpec((rows, DV), lambda i: (i, 0)),
        ),
        scratch_shapes=[pltpu.VMEM((DV, DK), F32)],
        cost_estimate=pl.CostEstimate(
            flops=20 * length * width * (3 * DK + 3 * DV), bytes_accessed=2 * length * width, transcendentals=0
        ),
        name="tokens",
    )(
        packed,
        block_scale,
        tokens,
        w_query,
        w_key,
        w_value,
        w_decay,
        w_rquery,
        w_gate,
        decay_rate.reshape(1, DK),
        query_gain.reshape(1, DV),
    )

    combined, squares = pl.pallas_call(
        reads_kernel,
        grid=(blocks,),
        out_shape=(
            jax.ShapeDtypeStruct((length, DV), F32),
            jax.ShapeDtypeStruct((tp_size, blocks, 1, BLK), F32),
        ),
        in_specs=[
            SMEM,
            ANY,
            pl.BlockSpec((BLK, DV), lambda i: (i, 0)),
            pl.BlockSpec((BLK, DV), lambda i: (i, 0)),
            pl.BlockSpec((BLK, DV), lambda i: (i, 0)),
        ],
        out_specs=(
            pl.BlockSpec((BLK, DV), lambda i: (i, 0)),
            pl.BlockSpec((tp_size, 1, 1, BLK), lambda i: (0, i, 0, 0)),
        ),
        scratch_shapes=[pltpu.VMEM((slots, plen, 2 * DV), BF16), pltpu.SemaphoreType.DMA((slots,))],
        name="reads",
    )(slot_index, got, read_query, gla, gate)
    everyone = lax.all_to_all(squares, "tp", split_axis=0, concat_axis=0, tiled=True)

    return pl.pallas_call(
        scale_kernel,
        out_shape=jax.ShapeDtypeStruct((length, DV), BF16),
        in_specs=[VMEM, VMEM, VMEM],
        out_specs=VMEM,
        name="scale",
    )(everyone, combined, out_gain.reshape(1, DV))


def solution(mesh):
    return jax.shard_map(
        on_device,
        mesh=mesh,
        in_specs=(
            P(("grp", "st"), None),
            P(None, "tp"),
            P(None, "tp"),
            P(None, "tp"),
            P(None, "tp"),
            P("tp"),
            P(("grp", "st")),
            P(None, "tp"),
            P(None, "tp"),
            P(None, "tp"),
            P(None, "tp"),
            P(),
            P(),
            P("tp"),
            P(("grp", "st"), None, None),
            P(("grp", "st"), None),
        ),
        out_specs=P(("grp", "st"), "tp"),
        check_vma=False,
    )
```

```python
import functools

import jax
import jax.numpy as jnp
from jax import lax
from jax.experimental import pallas as pl
from jax.experimental.pallas import tpu as pltpu
from jax.sharding import PartitionSpec as P

HEADS = 8
DK = 64
DV = 128
BLK = 128
NPASS = 4
EPS = 1e-06
PRECISE = lax.Precision.HIGHEST
F32 = jnp.float32
BF16 = jnp.bfloat16
MIB = 2**20


def nt(a, b, precision=None):
    return lax.dot_general(a, b, (((1,), (1,)), ((), ())), precision=precision, preferred_element_type=F32)


def head_norm(values, gain_row):
    return values * lax.rsqrt(jnp.mean(values * values, axis=-1, keepdims=True) + EPS) * gain_row


def requests_kernel(here, most, ids_ref, wanted_ref, block_ref, count_ref):
    owners = count_ref.shape[0]
    for i in range(owners):
        count_ref[i] = 0
    passes, blocks = ids_ref.shape
    for b in range(blocks):
        for j in range(passes):
            wanted = ids_ref[j, b]
            owner = jnp.clip(lax.div(wanted, jnp.int32(here)), 0, owners - 1)
            rank = jnp.minimum(count_ref[owner], most - 1)
            count_ref[owner] = rank + 1
            wanted_ref[owner, rank] = wanted - owner * here
            block_ref[owner, rank] = b


def passages_kernel(store_ref, wk_ref, wv_ref, gain_ref, out_ref, rows_ref, weight_ref, sems):
    count, rows, width = store_ref.shape
    step = count // (sems.shape[0] - 2)

    def part(i):
        at = pl.ds(i * step, step)
        return pltpu.make_async_copy(store_ref.at[at], rows_ref.at[at], sems.at[2 + i])

    weights = (
        pltpu.make_async_copy(wk_ref, weight_ref.at[:, :DV], sems.at[0]),
        pltpu.make_async_copy(wv_ref, weight_ref.at[:, DV:], sems.at[1]),
    )
    for copy in weights:
        copy.start()
    for i in range(count // step):
        part(i).start()
    for copy in weights:
        copy.wait()
    for i in range(count // step):
        part(i).wait()
        at = slice(i * step, (i + 1) * step)
        made = jnp.dot(rows_ref[at].reshape(step * rows, width), weight_ref[...], preferred_element_type=F32)
        made = made.astype(BF16)
        keys = head_norm(made[:, :DV].astype(F32), gain_ref[...]).astype(BF16)
        out_ref[at, :, :DV] = keys.reshape(step, rows, DV)
        out_ref[at, :, DV:] = made[:, DV:].reshape(step, rows, DV)


def other_index(me, st_size, step, flip, sign):
    chips = st_size // 2
    return lax.rem(me // 2 + (step if sign > 0 else chips - step), chips) * 2 + lax.rem(me + flip, 2)


def pack_kernel(offsets, st_size, me_ref, wanted_ref, made_ref, *refs):
    out_refs, sems = refs[:-1], refs[-1]
    held = made_ref.shape[0]
    most = wanted_ref.shape[1]
    me = me_ref[0]
    copies = []
    for j, (step, flip) in enumerate(offsets):
        reader = other_index(me, st_size, step, flip, 1)
        for rank in range(most):
            row = jnp.clip(wanted_ref[reader, rank], 0, held - 1)
            copies.append(pltpu.make_async_copy(made_ref.at[row], out_refs[j].at[rank], sems.at[j * most + rank]))
            copies[-1].start()
    for copy in copies:
        copy.wait()


def tokens_kernel(
    after_ref,
    scale_ref,
    tok_ref,
    wq_ref,
    wk_ref,
    wv_ref,
    wd_ref,
    wr_ref,
    wg_ref,
    rate_ref,
    qgain_ref,
    gla_ref,
    gate_ref,
    rq_ref,
    state_ref,
):
    step = pl.program_id(0)

    @pl.when(step == 0)
    def _():
        state_ref[...] = jnp.zeros_like(state_ref)

    tokens = tok_ref[...]
    rows = tokens.shape[0]

    def times(w_ref):
        return jnp.dot(tokens, w_ref[...], preferred_element_type=F32)

    query = nt(tokens, wq_ref[...])
    key = nt(tokens, wk_ref[...])
    value = times(wv_ref)
    decay = nt(tokens, wd_ref[...])
    rq_ref[...] = head_norm(times(wr_ref), qgain_ref[...]).astype(BF16)
    gate_ref[...] = jax.nn.sigmoid(times(wg_ref))
    row_id = lax.broadcasted_iota(jnp.int32, (BLK, BLK), 0)
    col_id = lax.broadcasted_iota(jnp.int32, (BLK, BLK), 1)
    causal = row_id >= col_id
    lower = causal.astype(F32)
    for b in range(rows // BLK):
        at = slice(b * BLK, (b + 1) * BLK)
        log_decay = -2.0 * rate_ref[...] * jax.nn.sigmoid(decay[at]) * scale_ref[step * (rows // BLK) + b]
        total = jnp.dot(lower, log_decay, precision=PRECISE, preferred_element_type=F32)
        last = total[BLK - 1 : BLK]
        q_dec = query[at] * DK ** (-0.5) * jnp.exp(total)
        k_dec = key[at] * jnp.exp(-total)
        scores = jnp.where(causal, nt(q_dec, k_dec, PRECISE), 0.0)
        within = jnp.dot(scores, value[at], precision=PRECISE, preferred_element_type=F32)
        gla_ref[at] = within + nt(q_dec, state_ref[...], PRECISE)
        update = lax.dot_general(
            value[at],
            key[at] * jnp.exp(last - total),
            (((0,), (0,)), ((), ())),
            precision=PRECISE,
            preferred_element_type=F32,
        )
        state_ref[...] = state_ref[...] * jnp.exp(last) + update


def reads_kernel(offsets, st_size, me_ref, block_ref, rq_ref, gla_ref, gate_ref, *refs):
    got_refs = refs[: len(offsets)]
    out_ref, square_ref, top_ref, bottom_ref = refs[len(offsets) :]
    most = block_ref.shape[1]
    blocks = rq_ref.shape[0]
    me = me_ref[0]
    top_ref[...] = jnp.zeros_like(top_ref)
    bottom_ref[...] = jnp.zeros_like(bottom_ref)
    for j, (step, flip) in enumerate(offsets):
        owner = other_index(me, st_size, step, flip, -1)
        for rank in range(most):
            b = jnp.clip(block_ref[owner, rank], 0, blocks - 1)
            weight = jnp.exp(nt(rq_ref[b], got_refs[j][rank, :, :DV]) * DV ** (-0.5))
            bottom_ref[b] += weight
            top_ref[b] += jnp.dot(weight.astype(BF16), got_refs[j][rank, :, DV:], preferred_element_type=F32)
    ones = jnp.ones((8, DV), F32)
    for b in range(blocks):
        bottom = jnp.sum(bottom_ref[b], axis=-1, keepdims=True)
        combined = gla_ref[b] + gate_ref[b] * (top_ref[b] / bottom)
        out_ref[b] = combined
        sums = nt(ones, combined * combined, PRECISE)
        square_ref[:, b] = jnp.broadcast_to(sums[0:1].reshape(1, 1, BLK), (square_ref.shape[0], 1, BLK))


def scale_kernel(square_ref, combined_ref, gain_ref, out_ref):
    total = jnp.sum(square_ref[...], axis=0)[:, 0, :]
    scale = lax.rsqrt(total / (HEADS * DV) + EPS)
    columns = jnp.transpose(scale)
    for b in range(total.shape[0]):
        at = slice(b * BLK, (b + 1) * BLK)
        out_ref[at] = (combined_ref[at] * columns[:, b : b + 1] * gain_ref[...]).astype(BF16)


VMEM = pl.BlockSpec(memory_space=pltpu.VMEM)
SMEM = pl.BlockSpec(memory_space=pltpu.SMEM)
ANY = pl.BlockSpec(memory_space=pl.ANY)


def whole(shape):
    return pl.BlockSpec(shape, lambda i: (0,) * len(shape))


def on_device(
    tokens,
    w_query,
    w_key,
    w_value,
    w_decay,
    decay_rate,
    block_scale,
    w_rquery,
    w_gate,
    w_rkey,
    w_rvalue,
    query_gain,
    key_gain,
    out_gain,
    store,
    passage_ids,
):
    length, width = tokens.shape
    blocks = length // BLK
    held, plen, _ = store.shape
    st_size = lax.axis_size("st")
    tp_size = lax.axis_size("tp")
    requests = passage_ids.shape[0] * passage_ids.shape[1]
    owners = min(st_size, requests // 2)
    most = requests // owners
    chips = st_size // 2
    me = lax.axis_index("st").astype(jnp.int32).reshape(1)

    wanted, block_of = pl.pallas_call(
        functools.partial(requests_kernel, held, most),
        out_shape=(
            jax.ShapeDtypeStruct((st_size, most), jnp.int32),
            jax.ShapeDtypeStruct((st_size, most), jnp.int32),
        ),
        in_specs=[SMEM],
        out_specs=(SMEM, SMEM),
        scratch_shapes=[pltpu.SMEM((st_size,), jnp.int32)],
        compiler_params=pltpu.CompilerParams(vmem_limit_bytes=2 * MIB),
        name="requests",
    )(passage_ids.T)
    incoming = lax.all_to_all(wanted, "st", split_axis=0, concat_axis=0, tiled=True)

    parts = held // 2
    made = pl.pallas_call(
        passages_kernel,
        out_shape=jax.ShapeDtypeStruct((held, plen, 2 * DV), BF16),
        in_specs=[ANY, ANY, ANY, VMEM],
        out_specs=VMEM,
        scratch_shapes=[
            pltpu.VMEM(store.shape, BF16),
            pltpu.VMEM((width, 2 * DV), BF16),
            pltpu.SemaphoreType.DMA((2 + parts,)),
        ],
        cost_estimate=pl.CostEstimate(
            flops=2 * held * plen * width * 2 * DV,
            bytes_accessed=2 * held * plen * (width + 2 * DV),
            transcendentals=0,
        ),
        compiler_params=pltpu.CompilerParams(vmem_limit_bytes=56 * MIB),
        name="passages",
    )(store, w_rkey, w_rvalue, key_gain.reshape(1, DV))

    order = [(0, 1)]
    for step in range(1, chips // 2 + 1):
        for way in dict.fromkeys((step, chips - step)):
            order += [(way, 0), (way, 1)]
    offsets = tuple(order[1:] + order[:1] + [(0, 0)])
    packed = pl.pallas_call(
        functools.partial(pack_kernel, offsets, st_size),
        out_shape=tuple(jax.ShapeDtypeStruct((most, plen, 2 * DV), BF16) for _ in offsets),
        in_specs=[SMEM, SMEM, VMEM],
        out_specs=tuple(ANY for _ in offsets),
        scratch_shapes=[pltpu.SemaphoreType.DMA((most * len(offsets),))],
        compiler_params=pltpu.CompilerParams(vmem_limit_bytes=8 * MIB),
        name="pack",
    )(me, incoming, made)

    def sent(array, step, flip):
        pairs = [(2 * y + e, ((y + step) % chips) * 2 + (e + flip) % 2) for y in range(chips) for e in range(2)]
        return lax.ppermute(array, "st", pairs)

    got = [packed[j] if o == (0, 0) else sent(packed[j], *o) for j, o in enumerate(offsets)]

    rows = 2 * BLK
    gla, gate, read_query = pl.pallas_call(
        tokens_kernel,
        grid=(length // rows,),
        out_shape=(
            jax.ShapeDtypeStruct((length, DV), F32),
            jax.ShapeDtypeStruct((length, DV), F32),
            jax.ShapeDtypeStruct((length, DV), BF16),
        ),
        in_specs=[
            ANY,
            SMEM,
            pl.BlockSpec((rows, width), lambda i: (i, 0)),
            whole((DK, width)),
            whole((DK, width)),
            whole((width, DV)),
            whole((DK, width)),
            whole((width, DV)),
            whole((width, DV)),
            whole((1, DK)),
            whole((1, DV)),
        ],
        out_specs=(
            pl.BlockSpec((rows, DV), lambda i: (i, 0)),
            pl.BlockSpec((rows, DV), lambda i: (i, 0)),
            pl.BlockSpec((rows, DV), lambda i: (i, 0)),
        ),
        scratch_shapes=[pltpu.VMEM((DV, DK), F32)],
        cost_estimate=pl.CostEstimate(
            flops=20 * length * width * (3 * DK + 3 * DV), bytes_accessed=2 * length * width, transcendentals=0
        ),
        compiler_params=pltpu.CompilerParams(vmem_limit_bytes=52 * MIB),
        name="tokens",
    )(
        packed[-1],
        block_scale,
        tokens,
        w_query.T,
        w_key.T,
        w_value,
        w_decay.T,
        w_rquery,
        w_gate,
        decay_rate.reshape(1, DK),
        query_gain.reshape(1, DV),
    )

    combined, squares = pl.pallas_call(
        functools.partial(reads_kernel, offsets, st_size),
        out_shape=(
            jax.ShapeDtypeStruct((blocks, BLK, DV), F32),
            jax.ShapeDtypeStruct((tp_size, blocks, 1, BLK), F32),
        ),
        in_specs=[SMEM, SMEM, VMEM, VMEM, VMEM] + [VMEM] * len(offsets),
        out_specs=(VMEM, VMEM),
        scratch_shapes=[pltpu.VMEM((blocks, BLK, DV), F32), pltpu.VMEM((blocks, BLK, DV), F32)],
        compiler_params=pltpu.CompilerParams(vmem_limit_bytes=14 * MIB),
        name="reads",
    )(
        me,
        block_of,
        read_query.reshape(blocks, BLK, DV),
        gla.reshape(blocks, BLK, DV),
        gate.reshape(blocks, BLK, DV),
        *got,
    )
    everyone = lax.all_to_all(squares, "tp", split_axis=0, concat_axis=0, tiled=True)

    return pl.pallas_call(
        scale_kernel,
        out_shape=jax.ShapeDtypeStruct((length, DV), BF16),
        in_specs=[VMEM, VMEM, VMEM],
        out_specs=VMEM,
        compiler_params=pltpu.CompilerParams(vmem_limit_bytes=8 * MIB),
        name="scale",
    )(everyone, combined.reshape(length, DV), out_gain.reshape(1, DV))


def solution(mesh):
    return jax.shard_map(
        on_device,
        mesh=mesh,
        in_specs=(
            P(("grp", "st"), None),
            P(None, "tp"),
            P(None, "tp"),
            P(None, "tp"),
            P(None, "tp"),
            P("tp"),
            P(("grp", "st")),
            P(None, "tp"),
            P(None, "tp"),
            P(None, "tp"),
            P(None, "tp"),
            P(),
            P(),
            P("tp"),
            P(("grp", "st"), None, None),
            P(("grp", "st"), None),
        ),
        out_specs=P(("grp", "st"), "tp"),
        check_vma=False,
    )
```

```python
import functools

import jax
import jax.numpy as jnp
from jax import lax
from jax.experimental import pallas as pl
from jax.experimental.pallas import tpu as pltpu
from jax.sharding import PartitionSpec as P

HEADS = 8
DK = 64
DV = 128
BLK = 128
NPASS = 4
EPS = 1e-06
PRECISE = lax.Precision.HIGHEST
F32 = jnp.float32
BF16 = jnp.bfloat16
MIB = 2**20
GROUP = 16
FAR = 3


def nt(a, b, precision=None):
    return lax.dot_general(a, b, (((1,), (1,)), ((), ())), precision=precision, preferred_element_type=F32)


def head_norm(values, gain_row):
    return values * lax.rsqrt(jnp.mean(values * values, axis=-1, keepdims=True) + EPS) * gain_row


def requests_kernel(here, most, ids_ref, wanted_ref, block_ref, count_ref):
    owners = count_ref.shape[0]
    for i in range(owners):
        count_ref[i] = 0
    passes, blocks = ids_ref.shape
    for b in range(blocks):
        for j in range(passes):
            wanted = ids_ref[j, b]
            owner = jnp.clip(lax.div(wanted, jnp.int32(here)), 0, owners - 1)
            rank = jnp.minimum(count_ref[owner], most - 1)
            count_ref[owner] = rank + 1
            wanted_ref[owner, rank] = wanted - owner * here
            block_ref[owner, rank] = b


def passages_kernel(store_ref, wk_ref, wv_ref, gain_ref, out_ref, weight_ref):
    count, rows, width = store_ref.shape
    weight_ref[:, :DV] = wk_ref[...]
    weight_ref[:, DV:] = wv_ref[...]
    made = jnp.dot(store_ref[...].reshape(count * rows, width), weight_ref[...], preferred_element_type=F32)
    made = made.astype(BF16)
    keys = head_norm(made[:, :DV].astype(F32), gain_ref[...]).astype(BF16)
    out_ref[:, :, :DV] = keys.reshape(count, rows, DV)
    out_ref[:, :, DV:] = made[:, DV:].reshape(count, rows, DV)


def other_index(me, st_size, step, flip, sign):
    chips = st_size // 2
    return lax.rem(me // 2 + (step if sign > 0 else chips - step), chips) * 2 + lax.rem(me + flip, 2)


def pack_kernel(offsets, st_size, me_ref, wanted_ref, made_ref, *out_refs):
    held = made_ref.shape[0]
    me = me_ref[0]
    for j, (step, flip) in enumerate(offsets):
        reader = other_index(me, st_size, step, flip, 1)
        for rank in range(wanted_ref.shape[1]):
            row = jnp.clip(wanted_ref[reader, rank], 0, held - 1)
            out_refs[j][rank] = made_ref[row]


def tokens_kernel(
    after_ref,
    scale_ref,
    tok_ref,
    wq_ref,
    wk_ref,
    wd_ref,
    wv_ref,
    wr_ref,
    wg_ref,
    rate_ref,
    qgain_ref,
    gla_ref,
    gate_ref,
    rq_ref,
    narrow_ref,
    wide_ref,
    state_ref,
):
    step = pl.program_id(0)

    @pl.when(step == 0)
    def _():
        state_ref[...] = jnp.zeros_like(state_ref)
        narrow_ref[:DK] = wq_ref[...]
        narrow_ref[DK : 2 * DK] = wk_ref[...]
        narrow_ref[2 * DK :] = wd_ref[...]
        wide_ref[:, :DV] = wv_ref[...]
        wide_ref[:, DV:] = wr_ref[...]

    tokens = tok_ref[...]
    blocks = tokens.shape[0] // BLK
    narrow = nt(tokens, narrow_ref[...])
    wide = jnp.dot(tokens, wide_ref[...], preferred_element_type=F32)
    gate_ref[...] = jax.nn.sigmoid(jnp.dot(tokens, wg_ref[...], preferred_element_type=F32))
    rq_ref[...] = head_norm(wide[:, DV:], qgain_ref[...]).astype(BF16)
    row_id = lax.broadcasted_iota(jnp.int32, (BLK, BLK), 0)
    col_id = lax.broadcasted_iota(jnp.int32, (BLK, BLK), 1)
    causal = row_id >= col_id
    lower = causal.astype(F32)
    places = [slice(b * BLK, (b + 1) * BLK) for b in range(blocks)]
    totals = []
    for b, at in enumerate(places):
        log_decay = -2.0 * rate_ref[...] * jax.nn.sigmoid(narrow[at, 2 * DK :]) * scale_ref[step * blocks + b]
        totals.append(jnp.dot(lower, log_decay, precision=PRECISE, preferred_element_type=F32))
    parts = []
    for at, total in zip(places, totals):
        key = narrow[at, DK : 2 * DK]
        q_dec = narrow[at, :DK] * DK ** (-0.5) * jnp.exp(total)
        k_dec = key * jnp.exp(-total)
        scores = jnp.where(causal, nt(q_dec, k_dec, PRECISE), 0.0)
        parts.append((q_dec, scores, key * jnp.exp(total[BLK - 1 :] - total)))
    inner = []
    for at, (_, scores, k_end) in zip(places, parts):
        value = wide[at, :DV]
        within = jnp.dot(scores, value, precision=PRECISE, preferred_element_type=F32)
        update = lax.dot_general(
            value, k_end, (((0,), (0,)), ((), ())), precision=PRECISE, preferred_element_type=F32
        )
        inner.append((within, update))
    for at, total, (q_dec, _, _), (within, update) in zip(places, totals, parts, inner):
        gla_ref[at] = within + nt(q_dec, state_ref[...], PRECISE)
        state_ref[...] = state_ref[...] * jnp.exp(total[BLK - 1 :]) + update


def add_reads(offsets, st_size, me_ref, block_ref, rq_ref, got_refs, top_ref, bottom_ref):
    blocks = rq_ref.shape[0]
    me = me_ref[0]
    items = []
    for j, (step, flip) in enumerate(offsets):
        owner = other_index(me, st_size, step, flip, -1)
        for rank in range(block_ref.shape[1]):
            items.append((got_refs[j], rank, jnp.clip(block_ref[owner, rank], 0, blocks - 1)))
    for first in range(0, len(items), GROUP):
        group = items[first : first + GROUP]
        scores = [nt(rq_ref[b], ref[rank, :, :DV]) for ref, rank, b in group]
        weights = [jnp.exp(score * DV ** (-0.5)) for score in scores]
        reads = [
            jnp.dot(weight.astype(BF16), ref[rank, :, DV:], preferred_element_type=F32)
            for weight, (ref, rank, _) in zip(weights, group)
        ]
        for weight, read, (_, _, b) in zip(weights, reads, group):
            bottom_ref[b] += weight
            top_ref[b] += read


def early_kernel(offsets, st_size, me_ref, block_ref, rq_ref, *refs):
    got_refs, (top_ref, bottom_ref) = refs[:-2], refs[-2:]
    top_ref[...] = jnp.zeros_like(top_ref)
    bottom_ref[...] = jnp.zeros_like(bottom_ref)
    add_reads(offsets, st_size, me_ref, block_ref, rq_ref, got_refs, top_ref, bottom_ref)


def late_kernel(offsets, st_size, me_ref, block_ref, rq_ref, gla_ref, gate_ref, top_in_ref, bottom_in_ref, *refs):
    got_refs = refs[: len(offsets)]
    out_ref, square_ref, top_ref, bottom_ref = refs[len(offsets) :]
    top_ref[...] = top_in_ref[...]
    bottom_ref[...] = bottom_in_ref[...]
    add_reads(offsets, st_size, me_ref, block_ref, rq_ref, got_refs, top_ref, bottom_ref)
    ones = jnp.ones((8, DV), F32)
    for b in range(rq_ref.shape[0]):
        bottom = jnp.sum(bottom_ref[b], axis=-1, keepdims=True)
        combined = gla_ref[b] + gate_ref[b] * (top_ref[b] / bottom)
        out_ref[b] = combined
        sums = nt(ones, combined * combined, PRECISE)
        square_ref[:, b] = jnp.broadcast_to(sums[0:1].reshape(1, 1, BLK), (square_ref.shape[0], 1, BLK))


def scale_kernel(square_ref, combined_ref, gain_ref, out_ref):
    total = jnp.sum(square_ref[...], axis=0)[:, 0, :]
    scale = lax.rsqrt(total / (HEADS * DV) + EPS)
    columns = jnp.transpose(scale)
    for b in range(total.shape[0]):
        at = slice(b * BLK, (b + 1) * BLK)
        out_ref[at] = (combined_ref[at] * columns[:, b : b + 1] * gain_ref[...]).astype(BF16)


VMEM = pl.BlockSpec(memory_space=pltpu.VMEM)
SMEM = pl.BlockSpec(memory_space=pltpu.SMEM)
ANY = pl.BlockSpec(memory_space=pl.ANY)


def whole(shape):
    return pl.BlockSpec(shape, lambda i: (0,) * len(shape))


def on_device(
    tokens,
    w_query,
    w_key,
    w_value,
    w_decay,
    decay_rate,
    block_scale,
    w_rquery,
    w_gate,
    w_rkey,
    w_rvalue,
    query_gain,
    key_gain,
    out_gain,
    store,
    passage_ids,
):
    length, width = tokens.shape
    blocks = length // BLK
    held, plen, _ = store.shape
    st_size = lax.axis_size("st")
    tp_size = lax.axis_size("tp")
    requests = passage_ids.shape[0] * passage_ids.shape[1]
    owners = min(st_size, requests // 2)
    most = requests // owners
    chips = st_size // 2
    me = lax.axis_index("st").astype(jnp.int32).reshape(1)

    wanted, block_of = pl.pallas_call(
        functools.partial(requests_kernel, held, most),
        out_shape=(
            jax.ShapeDtypeStruct((st_size, most), jnp.int32),
            jax.ShapeDtypeStruct((st_size, most), jnp.int32),
        ),
        in_specs=[SMEM],
        out_specs=(SMEM, SMEM),
        scratch_shapes=[pltpu.SMEM((st_size,), jnp.int32)],
        cost_estimate=pl.CostEstimate(flops=64 * held * plen * width * DV, bytes_accessed=0, transcendentals=0),
        compiler_params=pltpu.CompilerParams(vmem_limit_bytes=2 * MIB),
        name="requests",
    )(passage_ids.T)
    incoming = lax.all_to_all(wanted, "st", split_axis=0, concat_axis=0, tiled=True)

    made = pl.pallas_call(
        passages_kernel,
        out_shape=jax.ShapeDtypeStruct((held, plen, 2 * DV), BF16),
        in_specs=[VMEM, VMEM, VMEM, VMEM],
        out_specs=VMEM,
        scratch_shapes=[pltpu.VMEM((width, 2 * DV), BF16)],
        cost_estimate=pl.CostEstimate(
            flops=2 * held * plen * width * 2 * DV,
            bytes_accessed=2 * held * plen * (width + 2 * DV),
            transcendentals=0,
        ),
        compiler_params=pltpu.CompilerParams(vmem_limit_bytes=24 * MIB),
        name="passages",
    )(store, w_rkey, w_rvalue, key_gain.reshape(1, DV))

    order = [(0, 1)]
    for step in range(1, chips // 2 + 1):
        for way in dict.fromkeys((step, chips - step)):
            order += [(way, 0), (way, 1)]
    offsets = tuple(order[1:] + order[:1] + [(0, 0)])
    packed = pl.pallas_call(
        functools.partial(pack_kernel, offsets, st_size),
        out_shape=tuple(jax.ShapeDtypeStruct((most, plen, 2 * DV), BF16) for _ in offsets),
        in_specs=[SMEM, SMEM, VMEM],
        out_specs=tuple(VMEM for _ in offsets),
        compiler_params=pltpu.CompilerParams(vmem_limit_bytes=8 * MIB),
        name="pack",
    )(me, incoming, made)

    def sent(array, step, flip):
        pairs = [(2 * y + e, ((y + step) % chips) * 2 + (e + flip) % 2) for y in range(chips) for e in range(2)]
        return lax.ppermute(array, "st", pairs)

    got = [packed[j] if o == (0, 0) else sent(packed[j], *o) for j, o in enumerate(offsets)]

    rows = 4 * BLK
    gla, gate, read_query = pl.pallas_call(
        tokens_kernel,
        grid=(length // rows,),
        out_shape=(
            jax.ShapeDtypeStruct((length, DV), F32),
            jax.ShapeDtypeStruct((length, DV), F32),
            jax.ShapeDtypeStruct((length, DV), BF16),
        ),
        in_specs=[
            ANY,
            SMEM,
            pl.BlockSpec((rows, width), lambda i: (i, 0)),
            whole((DK, width)),
            whole((DK, width)),
            whole((DK, width)),
            whole((width, DV)),
            whole((width, DV)),
            whole((width, DV)),
            whole((1, DK)),
            whole((1, DV)),
        ],
        out_specs=(
            pl.BlockSpec((rows, DV), lambda i: (i, 0)),
            pl.BlockSpec((rows, DV), lambda i: (i, 0)),
            pl.BlockSpec((rows, DV), lambda i: (i, 0)),
        ),
        scratch_shapes=[
            pltpu.VMEM((3 * DK, width), BF16),
            pltpu.VMEM((width, 2 * DV), BF16),
            pltpu.VMEM((DV, DK), F32),
        ],
        cost_estimate=pl.CostEstimate(
            flops=20 * length * width * (3 * DK + 3 * DV), bytes_accessed=2 * length * width, transcendentals=0
        ),
        compiler_params=pltpu.CompilerParams(vmem_limit_bytes=32 * MIB),
        name="tokens",
    )(
        packed[-1],
        block_scale,
        tokens,
        w_query.T,
        w_key.T,
        w_decay.T,
        w_value,
        w_rquery,
        w_gate,
        decay_rate.reshape(1, DK),
        query_gain.reshape(1, DV),
    )

    blocked = (blocks, BLK, DV)
    read_query = read_query.reshape(blocked)
    sums = jax.ShapeDtypeStruct(blocked, F32)
    far = [j for j, (step, _) in enumerate(offsets) if min(step, chips - step) >= FAR]
    near = [j for j in range(len(offsets)) if j not in far]
    top, bottom = pl.pallas_call(
        functools.partial(early_kernel, tuple(offsets[j] for j in near), st_size),
        out_shape=(sums, sums),
        in_specs=[SMEM, SMEM, VMEM] + [VMEM] * len(near),
        out_specs=(VMEM, VMEM),
        cost_estimate=pl.CostEstimate(
            flops=8 * len(near) * most * BLK * plen * DV, bytes_accessed=0, transcendentals=0
        ),
        compiler_params=pltpu.CompilerParams(vmem_limit_bytes=14 * MIB),
        name="early",
    )(me, block_of, read_query, *[got[j] for j in near])
    combined, squares = pl.pallas_call(
        functools.partial(late_kernel, tuple(offsets[j] for j in far), st_size),
        out_shape=(sums, jax.ShapeDtypeStruct((tp_size, blocks, 1, BLK), F32)),
        in_specs=[SMEM, SMEM] + [VMEM] * (5 + len(far)),
        out_specs=(VMEM, VMEM),
        scratch_shapes=[pltpu.VMEM(blocked, F32), pltpu.VMEM(blocked, F32)],
        compiler_params=pltpu.CompilerParams(vmem_limit_bytes=14 * MIB),
        name="late",
    )(
        me,
        block_of,
        read_query,
        gla.reshape(blocked),
        gate.reshape(blocked),
        top,
        bottom,
        *[got[j] for j in far],
    )
    everyone = lax.all_to_all(squares, "tp", split_axis=0, concat_axis=0, tiled=True)

    return pl.pallas_call(
        scale_kernel,
        out_shape=jax.ShapeDtypeStruct((length, DV), BF16),
        in_specs=[VMEM, VMEM, VMEM],
        out_specs=VMEM,
        compiler_params=pltpu.CompilerParams(vmem_limit_bytes=8 * MIB),
        name="scale",
    )(everyone, combined.reshape(length, DV), out_gain.reshape(1, DV))


def solution(mesh):
    return jax.shard_map(
        on_device,
        mesh=mesh,
        in_specs=(
            P(("grp", "st"), None),
            P(None, "tp"),
            P(None, "tp"),
            P(None, "tp"),
            P(None, "tp"),
            P("tp"),
            P(("grp", "st")),
            P(None, "tp"),
            P(None, "tp"),
            P(None, "tp"),
            P(None, "tp"),
            P(),
            P(),
            P("tp"),
            P(("grp", "st"), None, None),
            P(("grp", "st"), None),
        ),
        out_specs=P(("grp", "st"), "tp"),
        check_vma=False,
    )
```

```python
import functools

import jax
import jax.numpy as jnp
from jax import lax
from jax.experimental import pallas as pl
from jax.experimental.pallas import tpu as pltpu
from jax.sharding import PartitionSpec as P

HEADS = 8
DK = 64
DV = 128
BLK = 128
NPASS = 4
EPS = 1e-06
PRECISE = lax.Precision.HIGHEST
F32 = jnp.float32
BF16 = jnp.bfloat16
MIB = 2**20
GROUP = 16


def nt(a, b, precision=None):
    return lax.dot_general(a, b, (((1,), (1,)), ((), ())), precision=precision, preferred_element_type=F32)


def head_norm(values, gain_row):
    return values * lax.rsqrt(jnp.mean(values * values, axis=-1, keepdims=True) + EPS) * gain_row


def requests_kernel(here, most, ids_ref, wanted_ref, block_ref, count_ref):
    owners = count_ref.shape[0]
    for i in range(owners):
        count_ref[i] = 0
    passes, blocks = ids_ref.shape
    for b in range(blocks):
        for j in range(passes):
            wanted = ids_ref[j, b]
            owner = jnp.clip(lax.div(wanted, jnp.int32(here)), 0, owners - 1)
            rank = jnp.minimum(count_ref[owner], most - 1)
            count_ref[owner] = rank + 1
            wanted_ref[owner, rank] = wanted - owner * here
            block_ref[owner, rank] = b


def passages_kernel(store_ref, wk_ref, wv_ref, gain_ref, out_ref, weight_ref):
    count, rows, width = store_ref.shape
    weight_ref[:, :DV] = wk_ref[...]
    weight_ref[:, DV:] = wv_ref[...]
    made = jnp.dot(store_ref[...].reshape(count * rows, width), weight_ref[...], preferred_element_type=F32)
    made = made.astype(BF16)
    keys = head_norm(made[:, :DV].astype(F32), gain_ref[...]).astype(BF16)
    out_ref[:, :, :DV] = keys.reshape(count, rows, DV)
    out_ref[:, :, DV:] = made[:, DV:].reshape(count, rows, DV)


def other_index(me, st_size, step, flip, sign):
    chips = st_size // 2
    return lax.rem(me // 2 + (step if sign > 0 else chips - step), chips) * 2 + lax.rem(me + flip, 2)


def pack_kernel(offsets, st_size, me_ref, wanted_ref, made_ref, *out_refs):
    held = made_ref.shape[0]
    me = me_ref[0]
    for j, (step, flip) in enumerate(offsets):
        reader = other_index(me, st_size, step, flip, 1)
        for rank in range(wanted_ref.shape[1]):
            row = jnp.clip(wanted_ref[reader, rank], 0, held - 1)
            out_refs[j][rank] = made_ref[row]


def tokens_kernel(
    after_ref,
    scale_ref,
    tok_ref,
    wq_ref,
    wk_ref,
    wd_ref,
    wv_ref,
    wr_ref,
    wg_ref,
    rate_ref,
    qgain_ref,
    gla_ref,
    gate_ref,
    rq_ref,
    narrow_ref,
    wide_ref,
    state_ref,
):
    step = pl.program_id(0)

    @pl.when(step == 0)
    def _():
        state_ref[...] = jnp.zeros_like(state_ref)
        narrow_ref[:DK] = wq_ref[...]
        narrow_ref[DK : 2 * DK] = wk_ref[...]
        narrow_ref[2 * DK :] = wd_ref[...]
        wide_ref[:, :DV] = wv_ref[...]
        wide_ref[:, DV:] = wr_ref[...]

    tokens = tok_ref[...]
    blocks = tokens.shape[0] // BLK
    narrow = nt(tokens, narrow_ref[...])
    wide = jnp.dot(tokens, wide_ref[...], preferred_element_type=F32)
    gate_ref[...] = jax.nn.sigmoid(jnp.dot(tokens, wg_ref[...], preferred_element_type=F32))
    rq_ref[...] = head_norm(wide[:, DV:], qgain_ref[...]).astype(BF16)
    row_id = lax.broadcasted_iota(jnp.int32, (BLK, BLK), 0)
    col_id = lax.broadcasted_iota(jnp.int32, (BLK, BLK), 1)
    causal = row_id >= col_id
    lower = causal.astype(F32)
    places = [slice(b * BLK, (b + 1) * BLK) for b in range(blocks)]
    totals = []
    for b, at in enumerate(places):
        log_decay = -2.0 * rate_ref[...] * jax.nn.sigmoid(narrow[at, 2 * DK :]) * scale_ref[step * blocks + b]
        totals.append(jnp.dot(lower, log_decay, precision=PRECISE, preferred_element_type=F32))
    parts = []
    for at, total in zip(places, totals):
        key = narrow[at, DK : 2 * DK]
        q_dec = narrow[at, :DK] * DK ** (-0.5) * jnp.exp(total)
        k_dec = key * jnp.exp(-total)
        scores = jnp.where(causal, nt(q_dec, k_dec, PRECISE), 0.0)
        parts.append((q_dec, scores, key * jnp.exp(total[BLK - 1 :] - total)))
    inner = []
    for at, (_, scores, k_end) in zip(places, parts):
        value = wide[at, :DV]
        within = jnp.dot(scores, value, precision=PRECISE, preferred_element_type=F32)
        update = lax.dot_general(
            value, k_end, (((0,), (0,)), ((), ())), precision=PRECISE, preferred_element_type=F32
        )
        inner.append((within, update))
    for at, total, (q_dec, _, _), (within, update) in zip(places, totals, parts, inner):
        gla_ref[at] = within + nt(q_dec, state_ref[...], PRECISE)
        state_ref[...] = state_ref[...] * jnp.exp(total[BLK - 1 :]) + update


def add_reads(offsets, st_size, me_ref, block_ref, rq_ref, got_refs, top_ref, bottom_ref):
    blocks = rq_ref.shape[0]
    me = me_ref[0]
    items = []
    for j, (step, flip) in enumerate(offsets):
        owner = other_index(me, st_size, step, flip, -1)
        for rank in range(block_ref.shape[1]):
            items.append((got_refs[j], rank, jnp.clip(block_ref[owner, rank], 0, blocks - 1)))
    for first in range(0, len(items), GROUP):
        group = items[first : first + GROUP]
        scores = [nt(rq_ref[b], ref[rank, :, :DV]) for ref, rank, b in group]
        weights = [jnp.exp(score * DV ** (-0.5)) for score in scores]
        reads = [
            jnp.dot(weight.astype(BF16), ref[rank, :, DV:], preferred_element_type=F32)
            for weight, (ref, rank, _) in zip(weights, group)
        ]
        for weight, read, (_, _, b) in zip(weights, reads, group):
            bottom_ref[b] += weight
            top_ref[b] += read


def early_kernel(offsets, st_size, me_ref, block_ref, rq_ref, *refs):
    got_refs, (top_ref, bottom_ref) = refs[:-2], refs[-2:]
    top_ref[...] = jnp.zeros_like(top_ref)
    bottom_ref[...] = jnp.zeros_like(bottom_ref)
    add_reads(offsets, st_size, me_ref, block_ref, rq_ref, got_refs, top_ref, bottom_ref)


def late_kernel(offsets, st_size, me_ref, block_ref, rq_ref, gla_ref, gate_ref, top_in_ref, bottom_in_ref, *refs):
    got_refs = refs[: len(offsets)]
    out_ref, square_ref, top_ref, bottom_ref = refs[len(offsets) :]
    top_ref[...] = top_in_ref[...]
    bottom_ref[...] = bottom_in_ref[...]
    add_reads(offsets, st_size, me_ref, block_ref, rq_ref, got_refs, top_ref, bottom_ref)
    ones = jnp.ones((8, DV), F32)
    for b in range(rq_ref.shape[0]):
        bottom = jnp.sum(bottom_ref[b], axis=-1, keepdims=True)
        combined = gla_ref[b] + gate_ref[b] * (top_ref[b] / bottom)
        out_ref[b] = combined
        sums = nt(ones, combined * combined, PRECISE)
        square_ref[:, b] = jnp.broadcast_to(sums[0:1].reshape(1, 1, BLK), (square_ref.shape[0], 1, BLK))


def scale_kernel(square_ref, combined_ref, gain_ref, out_ref):
    total = jnp.sum(square_ref[...], axis=0)[:, 0, :]
    scale = lax.rsqrt(total / (HEADS * DV) + EPS)
    columns = jnp.transpose(scale)
    for b in range(total.shape[0]):
        at = slice(b * BLK, (b + 1) * BLK)
        out_ref[at] = (combined_ref[at] * columns[:, b : b + 1] * gain_ref[...]).astype(BF16)


VMEM = pl.BlockSpec(memory_space=pltpu.VMEM)
SMEM = pl.BlockSpec(memory_space=pltpu.SMEM)
ANY = pl.BlockSpec(memory_space=pl.ANY)


def whole(shape):
    return pl.BlockSpec(shape, lambda i: (0,) * len(shape))


def on_device(
    tokens,
    w_query,
    w_key,
    w_value,
    w_decay,
    decay_rate,
    block_scale,
    w_rquery,
    w_gate,
    w_rkey,
    w_rvalue,
    query_gain,
    key_gain,
    out_gain,
    store,
    passage_ids,
):
    length, width = tokens.shape
    blocks = length // BLK
    held, plen, _ = store.shape
    st_size = lax.axis_size("st")
    tp_size = lax.axis_size("tp")
    requests = passage_ids.shape[0] * passage_ids.shape[1]
    owners = min(st_size, requests // 2)
    most = requests // owners
    chips = st_size // 2
    me = lax.axis_index("st").astype(jnp.int32).reshape(1)

    wanted, block_of = pl.pallas_call(
        functools.partial(requests_kernel, held, most),
        out_shape=(
            jax.ShapeDtypeStruct((st_size, most), jnp.int32),
            jax.ShapeDtypeStruct((st_size, most), jnp.int32),
        ),
        in_specs=[SMEM],
        out_specs=(SMEM, SMEM),
        scratch_shapes=[pltpu.SMEM((st_size,), jnp.int32)],
        cost_estimate=pl.CostEstimate(flops=64 * held * plen * width * DV, bytes_accessed=0, transcendentals=0),
        compiler_params=pltpu.CompilerParams(vmem_limit_bytes=2 * MIB),
        name="requests",
    )(passage_ids.T)
    incoming = lax.all_to_all(wanted, "st", split_axis=0, concat_axis=0, tiled=True)

    made = pl.pallas_call(
        passages_kernel,
        out_shape=jax.ShapeDtypeStruct((held, plen, 2 * DV), BF16),
        in_specs=[VMEM, VMEM, VMEM, VMEM],
        out_specs=VMEM,
        scratch_shapes=[pltpu.VMEM((width, 2 * DV), BF16)],
        cost_estimate=pl.CostEstimate(
            flops=2 * held * plen * width * 2 * DV,
            bytes_accessed=2 * held * plen * (width + 2 * DV),
            transcendentals=0,
        ),
        compiler_params=pltpu.CompilerParams(vmem_limit_bytes=24 * MIB),
        name="passages",
    )(store, w_rkey, w_rvalue, key_gain.reshape(1, DV))

    half = chips // 2
    order = []
    for step in [*range(2, half + 1), 1]:
        ways = tuple(dict.fromkeys((step, chips - step)))
        order += [(way, flip) for flip in (0, 1) for way in ways]
    offsets = tuple(order + [(0, 1), (0, 0)])
    packed = pl.pallas_call(
        functools.partial(pack_kernel, offsets, st_size),
        out_shape=tuple(jax.ShapeDtypeStruct((most, plen, 2 * DV), BF16) for _ in offsets),
        in_specs=[SMEM, SMEM, VMEM],
        out_specs=tuple(VMEM for _ in offsets),
        compiler_params=pltpu.CompilerParams(vmem_limit_bytes=8 * MIB),
        name="pack",
    )(me, incoming, made)

    def sent(array, step, flip):
        pairs = [(2 * y + e, ((y + step) % chips) * 2 + (e + flip) % 2) for y in range(chips) for e in range(2)]
        return lax.ppermute(array, "st", pairs)

    got = [packed[j] if o == (0, 0) else sent(packed[j], *o) for j, o in enumerate(offsets)]

    rows = 4 * BLK
    gla, gate, read_query = pl.pallas_call(
        tokens_kernel,
        grid=(length // rows,),
        out_shape=(
            jax.ShapeDtypeStruct((length, DV), F32),
            jax.ShapeDtypeStruct((length, DV), F32),
            jax.ShapeDtypeStruct((length, DV), BF16),
        ),
        in_specs=[
            ANY,
            SMEM,
            pl.BlockSpec((rows, width), lambda i: (i, 0)),
            whole((DK, width)),
            whole((DK, width)),
            whole((DK, width)),
            whole((width, DV)),
            whole((width, DV)),
            whole((width, DV)),
            whole((1, DK)),
            whole((1, DV)),
        ],
        out_specs=(
            pl.BlockSpec((rows, DV), lambda i: (i, 0)),
            pl.BlockSpec((rows, DV), lambda i: (i, 0)),
            pl.BlockSpec((rows, DV), lambda i: (i, 0)),
        ),
        scratch_shapes=[
            pltpu.VMEM((3 * DK, width), BF16),
            pltpu.VMEM((width, 2 * DV), BF16),
            pltpu.VMEM((DV, DK), F32),
        ],
        cost_estimate=pl.CostEstimate(
            flops=20 * length * width * (3 * DK + 3 * DV), bytes_accessed=2 * length * width, transcendentals=0
        ),
        compiler_params=pltpu.CompilerParams(vmem_limit_bytes=51 * MIB),
        name="tokens",
    )(
        packed[-1],
        block_scale,
        tokens,
        w_query.T,
        w_key.T,
        w_decay.T,
        w_value,
        w_rquery,
        w_gate,
        decay_rate.reshape(1, DK),
        query_gain.reshape(1, DV),
    )

    blocked = (blocks, BLK, DV)
    read_query = read_query.reshape(blocked)
    sums = jax.ShapeDtypeStruct(blocked, F32)
    last = [j for j, (step, _) in enumerate(offsets) if min(step, chips - step) in (1, half)]
    first = [j for j in range(len(offsets)) if j not in last]
    top, bottom = pl.pallas_call(
        functools.partial(early_kernel, tuple(offsets[j] for j in first), st_size),
        out_shape=(sums, sums),
        in_specs=[SMEM, SMEM, VMEM] + [VMEM] * len(first),
        out_specs=(VMEM, VMEM),
        cost_estimate=pl.CostEstimate(
            flops=8 * len(first) * most * BLK * plen * DV, bytes_accessed=0, transcendentals=0
        ),
        compiler_params=pltpu.CompilerParams(vmem_limit_bytes=14 * MIB),
        name="early",
    )(me, block_of, read_query, *[got[j] for j in first])
    combined, squares = pl.pallas_call(
        functools.partial(late_kernel, tuple(offsets[j] for j in last), st_size),
        out_shape=(sums, jax.ShapeDtypeStruct((tp_size, blocks, 1, BLK), F32)),
        in_specs=[SMEM, SMEM] + [VMEM] * (5 + len(last)),
        out_specs=(VMEM, VMEM),
        scratch_shapes=[pltpu.VMEM(blocked, F32), pltpu.VMEM(blocked, F32)],
        compiler_params=pltpu.CompilerParams(vmem_limit_bytes=14 * MIB),
        name="late",
    )(
        me,
        block_of,
        read_query,
        gla.reshape(blocked),
        gate.reshape(blocked),
        top,
        bottom,
        *[got[j] for j in last],
    )
    everyone = lax.all_to_all(squares, "tp", split_axis=0, concat_axis=0, tiled=True)

    return pl.pallas_call(
        scale_kernel,
        out_shape=jax.ShapeDtypeStruct((length, DV), BF16),
        in_specs=[VMEM, VMEM, VMEM],
        out_specs=VMEM,
        compiler_params=pltpu.CompilerParams(vmem_limit_bytes=8 * MIB),
        name="scale",
    )(everyone, combined.reshape(length, DV), out_gain.reshape(1, DV))


def solution(mesh):
    return jax.shard_map(
        on_device,
        mesh=mesh,
        in_specs=(
            P(("grp", "st"), None),
            P(None, "tp"),
            P(None, "tp"),
            P(None, "tp"),
            P(None, "tp"),
            P("tp"),
            P(("grp", "st")),
            P(None, "tp"),
            P(None, "tp"),
            P(None, "tp"),
            P(None, "tp"),
            P(),
            P(),
            P("tp"),
            P(("grp", "st"), None, None),
            P(("grp", "st"), None),
        ),
        out_specs=P(("grp", "st"), "tp"),
        check_vma=False,
    )
```

```python
import functools

import jax
import jax.numpy as jnp
from jax import lax
from jax.experimental import pallas as pl
from jax.experimental.pallas import tpu as pltpu
from jax.sharding import PartitionSpec as P


HEADS = 8
DK = 64
DV = 128
BLK = 128
EPS = 1e-06
PRECISE = lax.Precision.HIGHEST
F32 = jnp.float32
BF16 = jnp.bfloat16
MIB = 2**20
GROUP = 16


def nt(a, b, precision=None):
    return lax.dot_general(a, b, (((1,), (1,)), ((), ())), precision=precision, preferred_element_type=F32)


def head_norm(values, gain_row):
    return values * lax.rsqrt(jnp.mean(values * values, axis=-1, keepdims=True) + EPS) * gain_row


def requests_kernel(here, most, ids_ref, wanted_ref, block_ref, count_ref):
    owners = count_ref.shape[0]
    for i in range(owners):
        count_ref[i] = 0
    passes, blocks = ids_ref.shape
    for b in range(blocks):
        for j in range(passes):
            wanted = ids_ref[j, b]
            owner = jnp.clip(lax.div(wanted, jnp.int32(here)), 0, owners - 1)
            rank = jnp.minimum(count_ref[owner], most - 1)
            count_ref[owner] = rank + 1
            core = lax.rem(owner, 2)
            for other in range(2):
                wanted_ref[owner - core + other, core * most + rank] = wanted - owner * here
            block_ref[owner, rank] = b


def passages_kernel(store_ref, wk_ref, wv_ref, gain_ref, out_ref, weight_ref):
    count, rows, width = store_ref.shape
    weight_ref[:, :DV] = wk_ref[...]
    weight_ref[:, DV:] = wv_ref[...]
    made = jnp.dot(store_ref[...].reshape(count * rows, width), weight_ref[...], preferred_element_type=F32)
    made = made.astype(BF16)
    keys = head_norm(made[:, :DV].astype(F32), gain_ref[...]).astype(BF16)
    out_ref[:, :, :DV] = keys.reshape(count, rows, DV)
    out_ref[:, :, DV:] = made[:, DV:].reshape(count, rows, DV)


def chip_at(me, st_size, step):
    return lax.rem(me // 2 + step, st_size // 2)


def pack_kernel(steps, st_size, me_ref, wanted_ref, made_ref, beside_ref, *out_refs):
    held = made_ref.shape[0]
    me = me_ref[0]
    core = lax.rem(me, 2)
    most = wanted_ref.shape[1] // 2
    for j, step in enumerate(steps):
        reader = chip_at(me, st_size, step) * 2 + core
        for owner_core in range(2):
            for rank in range(most):
                at = owner_core * most + rank
                row = jnp.clip(wanted_ref[reader, at], 0, held - 1)
                out_refs[j][at] = jnp.where(core == owner_core, made_ref[row], beside_ref[row])


def tokens_kernel(
    after_ref,
    scale_ref,
    tok_ref,
    wq_ref,
    wk_ref,
    wd_ref,
    wv_ref,
    wr_ref,
    wg_ref,
    rate_ref,
    qgain_ref,
    gla_ref,
    gate_ref,
    rq_ref,
    narrow_ref,
    wide_ref,
    state_ref,
):
    step = pl.program_id(0)

    @pl.when(step == 0)
    def _():
        state_ref[...] = jnp.zeros_like(state_ref)
        narrow_ref[:DK] = wq_ref[...]
        narrow_ref[DK : 2 * DK] = wk_ref[...]
        narrow_ref[2 * DK :] = wd_ref[...]
        wide_ref[:, :DV] = wv_ref[...]
        wide_ref[:, DV:] = wr_ref[...]

    tokens = tok_ref[...]
    blocks = tokens.shape[0] // BLK
    narrow = nt(tokens, narrow_ref[...])
    wide = jnp.dot(tokens, wide_ref[...], preferred_element_type=F32)
    gate_ref[...] = jax.nn.sigmoid(jnp.dot(tokens, wg_ref[...], preferred_element_type=F32))
    rq_ref[...] = head_norm(wide[:, DV:], qgain_ref[...]).astype(BF16)
    row_id = lax.broadcasted_iota(jnp.int32, (BLK, BLK), 0)
    col_id = lax.broadcasted_iota(jnp.int32, (BLK, BLK), 1)
    causal = row_id >= col_id
    lower = causal.astype(F32)
    places = [slice(b * BLK, (b + 1) * BLK) for b in range(blocks)]
    totals = []
    for b, at in enumerate(places):
        log_decay = -2.0 * rate_ref[...] * jax.nn.sigmoid(narrow[at, 2 * DK :]) * scale_ref[step * blocks + b]
        totals.append(jnp.dot(lower, log_decay, precision=PRECISE, preferred_element_type=F32))
    parts = []
    for at, total in zip(places, totals):
        key = narrow[at, DK : 2 * DK]
        q_dec = narrow[at, :DK] * DK ** (-0.5) * jnp.exp(total)
        k_dec = key * jnp.exp(-total)
        scores = jnp.where(causal, nt(q_dec, k_dec, PRECISE), 0.0)
        parts.append((q_dec, scores, key * jnp.exp(total[BLK - 1 :] - total)))
    inner = []
    for at, (_, scores, k_end) in zip(places, parts):
        value = wide[at, :DV]
        within = jnp.dot(scores, value, precision=PRECISE, preferred_element_type=F32)
        update = lax.dot_general(
            value, k_end, (((0,), (0,)), ((), ())), precision=PRECISE, preferred_element_type=F32
        )
        inner.append((within, update))
    for at, total, (q_dec, _, _), (within, update) in zip(places, totals, parts, inner):
        gla_ref[at] = within + nt(q_dec, state_ref[...], PRECISE)
        state_ref[...] = state_ref[...] * jnp.exp(total[BLK - 1 :]) + update


def add_reads(steps, st_size, me_ref, block_ref, rq_ref, got_refs, top_ref, bottom_ref):
    blocks = rq_ref.shape[0]
    me = me_ref[0]
    most = block_ref.shape[1]
    items = []
    for j, step in enumerate(steps):
        chip = chip_at(me, st_size, st_size // 2 - step)
        for at in range(2 * most):
            block = jnp.clip(block_ref[chip * 2 + at // most, at % most], 0, blocks - 1)
            items.append((got_refs[j], at, block))
    for first in range(0, len(items), GROUP):
        group = items[first : first + GROUP]
        scores = [nt(rq_ref[b], ref[rank, :, :DV]) for ref, rank, b in group]
        weights = [jnp.exp(score * DV ** (-0.5)) for score in scores]
        reads = [
            jnp.dot(weight.astype(BF16), ref[rank, :, DV:], preferred_element_type=F32)
            for weight, (ref, rank, _) in zip(weights, group)
        ]
        for weight, read, (_, _, b) in zip(weights, reads, group):
            bottom_ref[b] += weight
            top_ref[b] += read


def early_kernel(steps, st_size, me_ref, block_ref, rq_ref, *refs):
    got_refs, (top_ref, bottom_ref) = refs[:-2], refs[-2:]
    top_ref[...] = jnp.zeros_like(top_ref)
    bottom_ref[...] = jnp.zeros_like(bottom_ref)
    add_reads(steps, st_size, me_ref, block_ref, rq_ref, got_refs, top_ref, bottom_ref)


def middle_kernel(steps, st_size, me_ref, block_ref, rq_ref, top_in_ref, bottom_in_ref, *refs):
    got_refs, (top_ref, bottom_ref) = refs[:-2], refs[-2:]
    top_ref[...] = top_in_ref[...]
    bottom_ref[...] = bottom_in_ref[...]
    add_reads(steps, st_size, me_ref, block_ref, rq_ref, got_refs, top_ref, bottom_ref)


def late_kernel(steps, st_size, me_ref, block_ref, rq_ref, gla_ref, gate_ref, top_in_ref, bottom_in_ref, *refs):
    got_refs = refs[: len(steps)]
    out_ref, square_ref, top_ref, bottom_ref = refs[len(steps) :]
    top_ref[...] = top_in_ref[...]
    bottom_ref[...] = bottom_in_ref[...]
    add_reads(steps, st_size, me_ref, block_ref, rq_ref, got_refs, top_ref, bottom_ref)
    ones = jnp.ones((8, DV), F32)
    for b in range(rq_ref.shape[0]):
        bottom = jnp.sum(bottom_ref[b], axis=-1, keepdims=True)
        combined = gla_ref[b] + gate_ref[b] * (top_ref[b] / bottom)
        out_ref[b] = combined
        sums = nt(ones, combined * combined, PRECISE)
        square_ref[:, b] = jnp.broadcast_to(sums[0:1].reshape(1, 1, BLK), (square_ref.shape[0], 1, BLK))


def scale_kernel(square_ref, combined_ref, gain_ref, out_ref):
    total = jnp.sum(square_ref[...], axis=0)[:, 0, :]
    scale = lax.rsqrt(total / (HEADS * DV) + EPS)
    columns = jnp.transpose(scale)
    for b in range(total.shape[0]):
        at = slice(b * BLK, (b + 1) * BLK)
        out_ref[at] = (combined_ref[at] * columns[:, b : b + 1] * gain_ref[...]).astype(BF16)


VMEM = pl.BlockSpec(memory_space=pltpu.VMEM)
SMEM = pl.BlockSpec(memory_space=pltpu.SMEM)
ANY = pl.BlockSpec(memory_space=pl.ANY)


def whole(shape):
    return pl.BlockSpec(shape, lambda i: (0,) * len(shape))


def on_device(
    tokens,
    w_query,
    w_key,
    w_value,
    w_decay,
    decay_rate,
    block_scale,
    w_rquery,
    w_gate,
    w_rkey,
    w_rvalue,
    query_gain,
    key_gain,
    out_gain,
    store,
    passage_ids,
):
    length, width = tokens.shape
    blocks = length // BLK
    held, plen, _ = store.shape
    st_size = lax.axis_size("st")
    tp_size = lax.axis_size("tp")
    requests = passage_ids.shape[0] * passage_ids.shape[1]
    owners = min(st_size, requests // 2)
    most = requests // owners
    chips = st_size // 2
    me = lax.axis_index("st").astype(jnp.int32).reshape(1)

    wanted, block_of = pl.pallas_call(
        functools.partial(requests_kernel, held, most),
        out_shape=(
            jax.ShapeDtypeStruct((st_size, 2 * most), jnp.int32),
            jax.ShapeDtypeStruct((st_size, most), jnp.int32),
        ),
        in_specs=[SMEM],
        out_specs=(SMEM, SMEM),
        scratch_shapes=[pltpu.SMEM((st_size,), jnp.int32)],
        cost_estimate=pl.CostEstimate(flops=64 * held * plen * width * DV, bytes_accessed=0, transcendentals=0),
        compiler_params=pltpu.CompilerParams(vmem_limit_bytes=2 * MIB),
        name="requests",
    )(passage_ids.T)
    incoming = lax.all_to_all(wanted, "st", split_axis=0, concat_axis=0, tiled=True)

    make = pl.pallas_call(
        passages_kernel,
        out_shape=jax.ShapeDtypeStruct((held, plen, 2 * DV), BF16),
        in_specs=[VMEM, VMEM, VMEM, VMEM],
        out_specs=VMEM,
        scratch_shapes=[pltpu.VMEM((width, 2 * DV), BF16)],
        cost_estimate=pl.CostEstimate(
            flops=2 * held * plen * width * 2 * DV,
            bytes_accessed=2 * held * plen * (width + 2 * DV),
            transcendentals=0,
        ),
        compiler_params=pltpu.CompilerParams(vmem_limit_bytes=24 * MIB),
        name="passages",
    )
    made = make(store, w_rkey, w_rvalue, key_gain.reshape(1, DV))

    def sent(array, step, flip):
        pairs = [(2 * y + e, ((y + step) % chips) * 2 + (e + flip) % 2) for y in range(chips) for e in range(2)]
        return lax.ppermute(array, "st", pairs)

    beside = sent(made, 0, 1)
    half = chips // 2
    steps = tuple(way for step in range(1, half + 1) for way in dict.fromkeys((step, chips - step))) + (0,)
    packed = pl.pallas_call(
        functools.partial(pack_kernel, steps, st_size),
        out_shape=tuple(jax.ShapeDtypeStruct((2 * most, plen, 2 * DV), BF16) for _ in steps),
        in_specs=[SMEM, SMEM, VMEM, VMEM],
        out_specs=tuple(VMEM for _ in steps),
        compiler_params=pltpu.CompilerParams(vmem_limit_bytes=8 * MIB),
        name="pack",
    )(me, incoming, made, beside)
    got = {step: sent(packed[j], step, 0) if step else packed[j] for j, step in enumerate(steps)}

    rows = 4 * BLK
    gla, gate, read_query = pl.pallas_call(
        tokens_kernel,
        grid=(length // rows,),
        out_shape=(
            jax.ShapeDtypeStruct((length, DV), F32),
            jax.ShapeDtypeStruct((length, DV), F32),
            jax.ShapeDtypeStruct((length, DV), BF16),
        ),
        in_specs=[
            ANY,
            SMEM,
            pl.BlockSpec((rows, width), lambda i: (i, 0)),
            whole((DK, width)),
            whole((DK, width)),
            whole((DK, width)),
            whole((width, DV)),
            whole((width, DV)),
            whole((width, DV)),
            whole((1, DK)),
            whole((1, DV)),
        ],
        out_specs=(
            pl.BlockSpec((rows, DV), lambda i: (i, 0)),
            pl.BlockSpec((rows, DV), lambda i: (i, 0)),
            pl.BlockSpec((rows, DV), lambda i: (i, 0)),
        ),
        scratch_shapes=[
            pltpu.VMEM((3 * DK, width), BF16),
            pltpu.VMEM((width, 2 * DV), BF16),
            pltpu.VMEM((DV, DK), F32),
        ],
        cost_estimate=pl.CostEstimate(
            flops=20 * length * width * (3 * DK + 3 * DV), bytes_accessed=2 * length * width, transcendentals=0
        ),
        compiler_params=pltpu.CompilerParams(vmem_limit_bytes=51 * MIB),
        name="tokens",
    )(
        packed[-1],
        block_scale,
        tokens,
        w_query.T,
        w_key.T,
        w_decay.T,
        w_value,
        w_rquery,
        w_gate,
        decay_rate.reshape(1, DK),
        query_gain.reshape(1, DV),
    )

    blocked = (blocks, BLK, DV)
    read_query = read_query.reshape(blocked)
    sums = jax.ShapeDtypeStruct(blocked, F32)
    away = {step: min(step, chips - step) for step in steps}
    groups = (
        tuple(step for step in steps if away[step] < half - 1),
        tuple(step for step in steps if away[step] == half - 1),
        tuple(step for step in steps if away[step] >= half),
    )

    def reads_cost(group):
        flops = 16 * len(group) * most * BLK * plen * DV
        return pl.CostEstimate(flops=flops, bytes_accessed=0, transcendentals=0)

    top, bottom = pl.pallas_call(
        functools.partial(early_kernel, groups[0], st_size),
        out_shape=(sums, sums),
        in_specs=[SMEM, SMEM] + [VMEM] * (1 + len(groups[0])),
        out_specs=(VMEM, VMEM),
        cost_estimate=reads_cost(groups[0]),
        compiler_params=pltpu.CompilerParams(vmem_limit_bytes=14 * MIB),
        name="early",
    )(me, block_of, read_query, *[got[step] for step in groups[0]])
    top, bottom = pl.pallas_call(
        functools.partial(middle_kernel, groups[1], st_size),
        out_shape=(sums, sums),
        in_specs=[SMEM, SMEM] + [VMEM] * (3 + len(groups[1])),
        out_specs=(VMEM, VMEM),
        cost_estimate=reads_cost(groups[1]),
        compiler_params=pltpu.CompilerParams(vmem_limit_bytes=14 * MIB),
        name="middle",
    )(me, block_of, read_query, top, bottom, *[got[step] for step in groups[1]])
    combined, squares = pl.pallas_call(
        functools.partial(late_kernel, groups[2], st_size),
        out_shape=(sums, jax.ShapeDtypeStruct((tp_size, blocks, 1, BLK), F32)),
        in_specs=[SMEM, SMEM] + [VMEM] * (5 + len(groups[2])),
        out_specs=(VMEM, VMEM),
        scratch_shapes=[pltpu.VMEM(blocked, F32), pltpu.VMEM(blocked, F32)],
        compiler_params=pltpu.CompilerParams(vmem_limit_bytes=14 * MIB),
        name="late",
    )(
        me,
        block_of,
        read_query,
        gla.reshape(blocked),
        gate.reshape(blocked),
        top,
        bottom,
        *[got[step] for step in groups[2]],
    )
    everyone = lax.all_to_all(squares, "tp", split_axis=0, concat_axis=0, tiled=True)

    return pl.pallas_call(
        scale_kernel,
        out_shape=jax.ShapeDtypeStruct((length, DV), BF16),
        in_specs=[VMEM, VMEM, VMEM],
        out_specs=VMEM,
        compiler_params=pltpu.CompilerParams(vmem_limit_bytes=8 * MIB),
        name="scale",
    )(everyone, combined.reshape(length, DV), out_gain.reshape(1, DV))


def solution(mesh):
    return jax.shard_map(
        on_device,
        mesh=mesh,
        in_specs=(
            P(("grp", "st"), None),
            P(None, "tp"),
            P(None, "tp"),
            P(None, "tp"),
            P(None, "tp"),
            P("tp"),
            P(("grp", "st")),
            P(None, "tp"),
            P(None, "tp"),
            P(None, "tp"),
            P(None, "tp"),
            P(),
            P(),
            P("tp"),
            P(("grp", "st"), None, None),
            P(("grp", "st"), None),
        ),
        out_specs=P(("grp", "st"), "tp"),
        check_vma=False,
    )
```

```python
import functools

import jax
import jax.numpy as jnp
from jax import lax
from jax.experimental import pallas as pl
from jax.experimental.pallas import tpu as pltpu
from jax.sharding import PartitionSpec as P

HEADS = 8
DK = 64
DV = 128
BLK = 128
NPASS = 4
EPS = 1e-06
PRECISE = lax.Precision.HIGHEST
F32 = jnp.float32
BF16 = jnp.bfloat16
MIB = 2**20
GROUP = 16
STRIDE = 4096


def nt(a, b, precision=None):
    return lax.dot_general(a, b, (((1,), (1,)), ((), ())), precision=precision, preferred_element_type=F32)


def head_norm(values, gain_row):
    return values * lax.rsqrt(jnp.mean(values * values, axis=-1, keepdims=True) + EPS) * gain_row


def requests_kernel(here, ids_ref, wanted_ref, block_ref):
    owners = wanted_ref.shape[0]
    passes, blocks = ids_ref.shape
    begin = here * lax.broadcasted_iota(jnp.int32, (owners, blocks), 0)
    column = lax.broadcasted_iota(jnp.int32, (owners, blocks), 1)
    low = jnp.full((owners, blocks), float(passes * blocks * STRIDE), F32)
    high = jnp.zeros((owners, blocks), F32)
    for j in range(passes):
        wanted = jnp.broadcast_to(ids_ref[j : j + 1, :], (owners, blocks))
        number = ((j * blocks + column) * STRIDE + wanted).astype(F32)
        asked = (wanted >= begin) & (wanted < begin + here)
        low = jnp.where(asked, jnp.minimum(low, number), low)
        high = jnp.where(asked, jnp.maximum(high, number), high)
    low = jnp.min(low, axis=1, keepdims=True).astype(jnp.int32)
    high = jnp.max(high, axis=1, keepdims=True).astype(jnp.int32)
    shape = wanted_ref.shape
    first = lax.broadcasted_iota(jnp.int32, shape, 1) == 0
    number = jnp.where(first, jnp.broadcast_to(low, shape), jnp.broadcast_to(high, shape))
    place = lax.shift_right_logical(number, STRIDE.bit_length() - 1)
    wanted_ref[...] = number - place * STRIDE - here * lax.broadcasted_iota(jnp.int32, shape, 0)
    block_ref[...] = lax.rem(place, blocks)


def passages_kernel(store_ref, wk_ref, wv_ref, gain_ref, out_ref, weight_ref):
    count, rows, width = store_ref.shape
    weight_ref[:, :DV] = wk_ref[...]
    weight_ref[:, DV:] = wv_ref[...]
    made = jnp.dot(store_ref[...].reshape(count * rows, width), weight_ref[...], preferred_element_type=F32)
    made = made.astype(BF16)
    keys = head_norm(made[:, :DV].astype(F32), gain_ref[...]).astype(BF16)
    out_ref[:, :, :DV] = keys.reshape(count, rows, DV)
    out_ref[:, :, DV:] = made[:, DV:].reshape(count, rows, DV)


def other_index(me, st_size, step, flip, sign):
    chips = st_size // 2
    return lax.rem(me // 2 + (step if sign > 0 else chips - step), chips) * 2 + lax.rem(me + flip, 2)


def pack_kernel(offsets, st_size, me_ref, wanted_ref, made_ref, *out_refs):
    held = made_ref.shape[0]
    me = me_ref[0]
    for j, (step, flip) in enumerate(offsets):
        reader = other_index(me, st_size, step, flip, 1)
        for rank in range(wanted_ref.shape[1]):
            row = jnp.clip(wanted_ref[reader, rank], 0, held - 1)
            out_refs[j][rank] = made_ref[row]


def tokens_kernel(
    after_ref,
    scale_ref,
    tok_ref,
    wq_ref,
    wk_ref,
    wd_ref,
    wv_ref,
    wr_ref,
    wg_ref,
    rate_ref,
    qgain_ref,
    gla_ref,
    gate_ref,
    rq_ref,
    narrow_ref,
    wide_ref,
    state_ref,
):
    step = pl.program_id(0)

    @pl.when(step == 0)
    def _():
        state_ref[...] = jnp.zeros_like(state_ref)
        narrow_ref[:DK] = wq_ref[...]
        narrow_ref[DK : 2 * DK] = wk_ref[...]
        narrow_ref[2 * DK :] = wd_ref[...]
        wide_ref[:, :DV] = wv_ref[...]
        wide_ref[:, DV:] = wr_ref[...]

    tokens = tok_ref[...]
    blocks = tokens.shape[0] // BLK
    narrow = nt(tokens, narrow_ref[...])
    wide = jnp.dot(tokens, wide_ref[...], preferred_element_type=F32)
    gate_ref[...] = jax.nn.sigmoid(jnp.dot(tokens, wg_ref[...], preferred_element_type=F32))
    rq_ref[...] = head_norm(wide[:, DV:], qgain_ref[...]).astype(BF16)
    row_id = lax.broadcasted_iota(jnp.int32, (BLK, BLK), 0)
    col_id = lax.broadcasted_iota(jnp.int32, (BLK, BLK), 1)
    causal = row_id >= col_id
    lower = causal.astype(F32)
    places = [slice(b * BLK, (b + 1) * BLK) for b in range(blocks)]
    totals = []
    for b, at in enumerate(places):
        log_decay = -2.0 * rate_ref[...] * jax.nn.sigmoid(narrow[at, 2 * DK :]) * scale_ref[step * blocks + b]
        totals.append(jnp.dot(lower, log_decay, precision=PRECISE, preferred_element_type=F32))
    parts = []
    for at, total in zip(places, totals):
        key = narrow[at, DK : 2 * DK]
        q_dec = narrow[at, :DK] * DK ** (-0.5) * jnp.exp(total)
        k_dec = key * jnp.exp(-total)
        scores = jnp.where(causal, nt(q_dec, k_dec, PRECISE), 0.0)
        parts.append((q_dec, scores, key * jnp.exp(total[BLK - 1 :] - total)))
    inner = []
    for at, (_, scores, k_end) in zip(places, parts):
        value = wide[at, :DV]
        within = jnp.dot(scores, value, precision=PRECISE, preferred_element_type=F32)
        update = lax.dot_general(
            value, k_end, (((0,), (0,)), ((), ())), precision=PRECISE, preferred_element_type=F32
        )
        inner.append((within, update))
    for at, total, (q_dec, _, _), (within, update) in zip(places, totals, parts, inner):
        gla_ref[at] = within + nt(q_dec, state_ref[...], PRECISE)
        state_ref[...] = state_ref[...] * jnp.exp(total[BLK - 1 :]) + update


def add_reads(offsets, st_size, me_ref, block_ref, rq_ref, got_refs, top_ref, bottom_ref):
    blocks = rq_ref.shape[0]
    me = me_ref[0]
    items = []
    for j, (step, flip) in enumerate(offsets):
        owner = other_index(me, st_size, step, flip, -1)
        for rank in range(block_ref.shape[1]):
            items.append((got_refs[j], rank, jnp.clip(block_ref[owner, rank], 0, blocks - 1)))
    for first in range(0, len(items), GROUP):
        group = items[first : first + GROUP]
        scores = [nt(rq_ref[b], ref[rank, :, :DV]) for ref, rank, b in group]
        weights = [jnp.exp(score * DV ** (-0.5)) for score in scores]
        reads = [
            jnp.dot(weight.astype(BF16), ref[rank, :, DV:], preferred_element_type=F32)
            for weight, (ref, rank, _) in zip(weights, group)
        ]
        for weight, read, (_, _, b) in zip(weights, reads, group):
            bottom_ref[b] += weight
            top_ref[b] += read


def early_kernel(offsets, st_size, me_ref, block_ref, rq_ref, *refs):
    got_refs, (top_ref, bottom_ref) = refs[:-2], refs[-2:]
    top_ref[...] = jnp.zeros_like(top_ref)
    bottom_ref[...] = jnp.zeros_like(bottom_ref)
    add_reads(offsets, st_size, me_ref, block_ref, rq_ref, got_refs, top_ref, bottom_ref)


def middle_kernel(offsets, st_size, me_ref, block_ref, rq_ref, top_in_ref, bottom_in_ref, *refs):
    got_refs, (top_ref, bottom_ref) = refs[:-2], refs[-2:]
    top_ref[...] = top_in_ref[...]
    bottom_ref[...] = bottom_in_ref[...]
    add_reads(offsets, st_size, me_ref, block_ref, rq_ref, got_refs, top_ref, bottom_ref)


def late_kernel(offsets, st_size, me_ref, block_ref, rq_ref, gla_ref, gate_ref, top_in_ref, bottom_in_ref, *refs):
    got_refs = refs[: len(offsets)]
    out_ref, square_ref, top_ref, bottom_ref = refs[len(offsets) :]
    top_ref[...] = top_in_ref[...]
    bottom_ref[...] = bottom_in_ref[...]
    add_reads(offsets, st_size, me_ref, block_ref, rq_ref, got_refs, top_ref, bottom_ref)
    ones = jnp.ones((8, DV), F32)
    for b in range(rq_ref.shape[0]):
        bottom = jnp.sum(bottom_ref[b], axis=-1, keepdims=True)
        combined = gla_ref[b] + gate_ref[b] * (top_ref[b] / bottom)
        out_ref[b] = combined
        sums = nt(ones, combined * combined, PRECISE)
        square_ref[:, b] = jnp.broadcast_to(sums[0:1].reshape(1, 1, BLK), (square_ref.shape[0], 1, BLK))


def scale_kernel(square_ref, combined_ref, gain_ref, out_ref):
    total = jnp.sum(square_ref[...], axis=0)[:, 0, :]
    scale = lax.rsqrt(total / (HEADS * DV) + EPS)
    columns = jnp.transpose(scale)
    for b in range(total.shape[0]):
        at = slice(b * BLK, (b + 1) * BLK)
        out_ref[at] = (combined_ref[at] * columns[:, b : b + 1] * gain_ref[...]).astype(BF16)


VMEM = pl.BlockSpec(memory_space=pltpu.VMEM)
SMEM = pl.BlockSpec(memory_space=pltpu.SMEM)
ANY = pl.BlockSpec(memory_space=pl.ANY)


def whole(shape):
    return pl.BlockSpec(shape, lambda i: (0,) * len(shape))


def on_device(
    tokens,
    w_query,
    w_key,
    w_value,
    w_decay,
    decay_rate,
    block_scale,
    w_rquery,
    w_gate,
    w_rkey,
    w_rvalue,
    query_gain,
    key_gain,
    out_gain,
    store,
    passage_ids,
):
    length, width = tokens.shape
    blocks = length // BLK
    held, plen, _ = store.shape
    st_size = lax.axis_size("st")
    tp_size = lax.axis_size("tp")
    requests = passage_ids.shape[0] * passage_ids.shape[1]
    owners = min(st_size, requests // 2)
    most = requests // owners
    chips = st_size // 2
    me = lax.axis_index("st").astype(jnp.int32).reshape(1)

    wanted, block_of = pl.pallas_call(
        functools.partial(requests_kernel, held),
        out_shape=(
            jax.ShapeDtypeStruct((st_size, most), jnp.int32),
            jax.ShapeDtypeStruct((st_size, most), jnp.int32),
        ),
        in_specs=[VMEM],
        out_specs=(VMEM, VMEM),
        cost_estimate=pl.CostEstimate(flops=64 * held * plen * width * DV, bytes_accessed=0, transcendentals=0),
        compiler_params=pltpu.CompilerParams(vmem_limit_bytes=2 * MIB),
        name="requests",
    )(passage_ids.T)
    incoming = lax.all_to_all(wanted, "st", split_axis=0, concat_axis=0, tiled=True)

    made = pl.pallas_call(
        passages_kernel,
        out_shape=jax.ShapeDtypeStruct((held, plen, 2 * DV), BF16),
        in_specs=[VMEM, VMEM, VMEM, VMEM],
        out_specs=VMEM,
        scratch_shapes=[pltpu.VMEM((width, 2 * DV), BF16)],
        cost_estimate=pl.CostEstimate(
            flops=2 * held * plen * width * 2 * DV,
            bytes_accessed=2 * held * plen * (width + 2 * DV),
            transcendentals=0,
        ),
        compiler_params=pltpu.CompilerParams(vmem_limit_bytes=24 * MIB),
        name="passages",
    )(store, w_rkey, w_rvalue, key_gain.reshape(1, DV))

    half = chips // 2
    order = []
    for step in [*range(2, half + 1), 1]:
        ways = tuple(dict.fromkeys((step, chips - step)))
        order += [(way, flip) for flip in (0, 1) for way in ways]
    offsets = tuple(order + [(0, 1), (0, 0)])
    packed = pl.pallas_call(
        functools.partial(pack_kernel, offsets, st_size),
        out_shape=tuple(jax.ShapeDtypeStruct((most, plen, 2 * DV), BF16) for _ in offsets),
        in_specs=[SMEM, SMEM, VMEM],
        out_specs=tuple(VMEM for _ in offsets),
        compiler_params=pltpu.CompilerParams(vmem_limit_bytes=8 * MIB),
        name="pack",
    )(me, incoming, made)

    def sent(array, step, flip):
        pairs = [(2 * y + e, ((y + step) % chips) * 2 + (e + flip) % 2) for y in range(chips) for e in range(2)]
        return lax.ppermute(array, "st", pairs)

    got = [packed[j] if o == (0, 0) else sent(packed[j], *o) for j, o in enumerate(offsets)]

    rows = 4 * BLK
    gla, gate, read_query = pl.pallas_call(
        tokens_kernel,
        grid=(length // rows,),
        out_shape=(
            jax.ShapeDtypeStruct((length, DV), F32),
            jax.ShapeDtypeStruct((length, DV), F32),
            jax.ShapeDtypeStruct((length, DV), BF16),
        ),
        in_specs=[
            ANY,
            SMEM,
            pl.BlockSpec((rows, width), lambda i: (i, 0)),
            whole((DK, width)),
            whole((DK, width)),
            whole((DK, width)),
            whole((width, DV)),
            whole((width, DV)),
            whole((width, DV)),
            whole((1, DK)),
            whole((1, DV)),
        ],
        out_specs=(
            pl.BlockSpec((rows, DV), lambda i: (i, 0)),
            pl.BlockSpec((rows, DV), lambda i: (i, 0)),
            pl.BlockSpec((rows, DV), lambda i: (i, 0)),
        ),
        scratch_shapes=[
            pltpu.VMEM((3 * DK, width), BF16),
            pltpu.VMEM((width, 2 * DV), BF16),
            pltpu.VMEM((DV, DK), F32),
        ],
        cost_estimate=pl.CostEstimate(
            flops=20 * length * width * (3 * DK + 3 * DV), bytes_accessed=2 * length * width, transcendentals=0
        ),
        compiler_params=pltpu.CompilerParams(vmem_limit_bytes=51 * MIB),
        name="tokens",
    )(
        packed[-1],
        block_scale,
        tokens,
        w_query.T,
        w_key.T,
        w_decay.T,
        w_value,
        w_rquery,
        w_gate,
        decay_rate.reshape(1, DK),
        query_gain.reshape(1, DV),
    )

    blocked = (blocks, BLK, DV)
    read_query = read_query.reshape(blocked)
    sums = jax.ShapeDtypeStruct(blocked, F32)
    last = [j for j, (step, _) in enumerate(offsets) if min(step, chips - step) == 1]
    middle = [j for j, (step, _) in enumerate(offsets) if step == half]
    first = [j for j in range(len(offsets)) if j not in last + middle]
    top, bottom = pl.pallas_call(
        functools.partial(early_kernel, tuple(offsets[j] for j in first), st_size),
        out_shape=(sums, sums),
        in_specs=[SMEM, SMEM, VMEM] + [VMEM] * len(first),
        out_specs=(VMEM, VMEM),
        cost_estimate=pl.CostEstimate(
            flops=8 * len(first) * most * BLK * plen * DV, bytes_accessed=0, transcendentals=0
        ),
        compiler_params=pltpu.CompilerParams(vmem_limit_bytes=14 * MIB),
        name="early",
    )(me, block_of, read_query, *[got[j] for j in first])
    top, bottom = pl.pallas_call(
        functools.partial(middle_kernel, tuple(offsets[j] for j in middle), st_size),
        out_shape=(sums, sums),
        in_specs=[SMEM, SMEM] + [VMEM] * (3 + len(middle)),
        out_specs=(VMEM, VMEM),
        cost_estimate=pl.CostEstimate(
            flops=8 * len(middle) * most * BLK * plen * DV, bytes_accessed=0, transcendentals=0
        ),
        compiler_params=pltpu.CompilerParams(vmem_limit_bytes=14 * MIB),
        name="middle",
    )(me, block_of, read_query, top, bottom, *[got[j] for j in middle])
    combined, squares = pl.pallas_call(
        functools.partial(late_kernel, tuple(offsets[j] for j in last), st_size),
        out_shape=(sums, jax.ShapeDtypeStruct((tp_size, blocks, 1, BLK), F32)),
        in_specs=[SMEM, SMEM] + [VMEM] * (5 + len(last)),
        out_specs=(VMEM, VMEM),
        scratch_shapes=[pltpu.VMEM(blocked, F32), pltpu.VMEM(blocked, F32)],
        compiler_params=pltpu.CompilerParams(vmem_limit_bytes=14 * MIB),
        name="late",
    )(
        me,
        block_of,
        read_query,
        gla.reshape(blocked),
        gate.reshape(blocked),
        top,
        bottom,
        *[got[j] for j in last],
    )
    everyone = lax.all_to_all(squares, "tp", split_axis=0, concat_axis=0, tiled=True)

    return pl.pallas_call(
        scale_kernel,
        out_shape=jax.ShapeDtypeStruct((length, DV), BF16),
        in_specs=[VMEM, VMEM, VMEM],
        out_specs=VMEM,
        compiler_params=pltpu.CompilerParams(vmem_limit_bytes=8 * MIB),
        name="scale",
    )(everyone, combined.reshape(length, DV), out_gain.reshape(1, DV))


def solution(mesh):
    return jax.shard_map(
        on_device,
        mesh=mesh,
        in_specs=(
            P(("grp", "st"), None),
            P(None, "tp"),
            P(None, "tp"),
            P(None, "tp"),
            P(None, "tp"),
            P("tp"),
            P(("grp", "st")),
            P(None, "tp"),
            P(None, "tp"),
            P(None, "tp"),
            P(None, "tp"),
            P(),
            P(),
            P("tp"),
            P(("grp", "st"), None, None),
            P(("grp", "st"), None),
        ),
        out_specs=P(("grp", "st"), "tp"),
        check_vma=False,
    )
```

```python
import functools

import jax
import jax.numpy as jnp
from jax import lax
from jax.experimental import pallas as pl
from jax.experimental.pallas import tpu as pltpu
from jax.sharding import PartitionSpec as P


HEADS = 8
DK = 64
DV = 128
BLK = 128
PLEN = 128
EPS = 1e-06
PRECISE = lax.Precision.HIGHEST
F32 = jnp.float32
BF16 = jnp.bfloat16
MIB = 2**20
GROUP = 16
LEAD = 2
STRIDE = 4096


def nt(a, b, precision=None):
    return lax.dot_general(a, b, (((1,), (1,)), ((), ())), precision=precision, preferred_element_type=F32)


def head_norm(values, gain_row):
    return values * lax.rsqrt(jnp.mean(values * values, axis=-1, keepdims=True) + EPS) * gain_row


def requests_kernel(here, ids_ref, wanted_ref, block_ref):
    owners = wanted_ref.shape[0]
    passes, blocks = ids_ref.shape
    begin = here * lax.broadcasted_iota(jnp.int32, (owners, blocks), 0)
    column = lax.broadcasted_iota(jnp.int32, (owners, blocks), 1)
    low = jnp.full((owners, blocks), float(passes * blocks * STRIDE), F32)
    high = jnp.zeros((owners, blocks), F32)
    for j in range(passes):
        wanted = jnp.broadcast_to(ids_ref[j : j + 1, :], (owners, blocks))
        number = ((j * blocks + column) * STRIDE + wanted).astype(F32)
        asked = (wanted >= begin) & (wanted < begin + here)
        low = jnp.where(asked, jnp.minimum(low, number), low)
        high = jnp.where(asked, jnp.maximum(high, number), high)
    low = jnp.min(low, axis=1, keepdims=True).astype(jnp.int32)
    high = jnp.max(high, axis=1, keepdims=True).astype(jnp.int32)
    shape = wanted_ref.shape
    first = lax.broadcasted_iota(jnp.int32, shape, 1) == 0
    number = jnp.where(first, jnp.broadcast_to(low, shape), jnp.broadcast_to(high, shape))
    place = lax.shift_right_logical(number, STRIDE.bit_length() - 1)
    wanted_ref[...] = number - place * STRIDE - here * lax.broadcasted_iota(jnp.int32, shape, 0)
    block_ref[...] = lax.rem(place, blocks)


def passages_kernel(store_ref, wk_ref, wv_ref, gain_ref, out_ref, weight_ref):
    count, rows, width = store_ref.shape
    weight_ref[:, :DV] = wk_ref[...]
    weight_ref[:, DV:] = wv_ref[...]
    made = jnp.dot(store_ref[...].reshape(count * rows, width), weight_ref[...], preferred_element_type=F32)
    made = made.astype(BF16)
    keys = head_norm(made[:, :DV].astype(F32), gain_ref[...]).astype(BF16)
    out_ref[:, :, :DV] = keys.reshape(count, rows, DV)
    out_ref[:, :, DV:] = made[:, DV:].reshape(count, rows, DV)


def other_index(me, st_size, step, flip, sign):
    chips = st_size // 2
    return lax.rem(me // 2 + (step if sign > 0 else chips - step), chips) * 2 + lax.rem(me + flip, 2)


def pack_kernel(offsets, st_size, me_ref, wanted_ref, made_ref, *out_refs):
    held = made_ref.shape[0]
    me = me_ref[0]
    for j, (step, flip) in enumerate(offsets):
        reader = other_index(me, st_size, step, flip, 1)
        for rank in range(wanted_ref.shape[1]):
            row = jnp.clip(wanted_ref[reader, rank], 0, held - 1)
            out_refs[j][rank] = made_ref[row]


def tokens_kernel(
    after_ref,
    scale_ref,
    tok_ref,
    wq_ref,
    wk_ref,
    wd_ref,
    wv_ref,
    wr_ref,
    wg_ref,
    rate_ref,
    qgain_ref,
    gla_ref,
    gate_ref,
    rq_ref,
    narrow_ref,
    wide_ref,
    state_ref,
):
    step = pl.program_id(0)

    @pl.when(step == 0)
    def _():
        state_ref[...] = jnp.zeros_like(state_ref)
        narrow_ref[:DK] = wq_ref[...]
        narrow_ref[DK : 2 * DK] = wk_ref[...]
        narrow_ref[2 * DK :] = wd_ref[...]
        wide_ref[:, :DV] = wv_ref[...]
        wide_ref[:, DV:] = wr_ref[...]

    tokens = tok_ref[...]
    blocks = tokens.shape[0] // BLK
    narrow = nt(tokens, narrow_ref[...])
    wide = jnp.dot(tokens, wide_ref[...], preferred_element_type=F32)
    gate_ref[...] = jax.nn.sigmoid(jnp.dot(tokens, wg_ref[...], preferred_element_type=F32))
    rq_ref[...] = head_norm(wide[:, DV:], qgain_ref[...]).astype(BF16)
    row_id = lax.broadcasted_iota(jnp.int32, (BLK, BLK), 0)
    col_id = lax.broadcasted_iota(jnp.int32, (BLK, BLK), 1)
    causal = row_id >= col_id
    lower = causal.astype(F32)
    places = [slice(b * BLK, (b + 1) * BLK) for b in range(blocks)]
    totals = []
    for b, at in enumerate(places):
        log_decay = -2.0 * rate_ref[...] * jax.nn.sigmoid(narrow[at, 2 * DK :]) * scale_ref[step * blocks + b]
        totals.append(jnp.dot(lower, log_decay, precision=PRECISE, preferred_element_type=F32))
    parts = []
    for at, total in zip(places, totals):
        key = narrow[at, DK : 2 * DK]
        q_dec = narrow[at, :DK] * DK ** (-0.5) * jnp.exp(total)
        k_dec = key * jnp.exp(-total)
        scores = jnp.where(causal, nt(q_dec, k_dec, PRECISE), 0.0)
        parts.append((q_dec, scores, key * jnp.exp(total[BLK - 1 :] - total)))
    inner = []
    for at, (_, scores, k_end) in zip(places, parts):
        value = wide[at, :DV]
        within = jnp.dot(scores, value, precision=PRECISE, preferred_element_type=F32)
        update = lax.dot_general(
            value, k_end, (((0,), (0,)), ((), ())), precision=PRECISE, preferred_element_type=F32
        )
        inner.append((within, update))
    for at, total, (q_dec, _, _), (within, update) in zip(places, totals, parts, inner):
        gla_ref[at] = within + nt(q_dec, state_ref[...], PRECISE)
        state_ref[...] = state_ref[...] * jnp.exp(total[BLK - 1 :]) + update


def add_reads(offsets, st_size, me_ref, block_ref, rq_ref, got_refs, top_ref, bottom_ref):
    ones = jnp.ones((PLEN, DV), BF16)
    blocks = rq_ref.shape[0]
    me = me_ref[0]
    items = []
    for j, (step, flip) in enumerate(offsets):
        owner = other_index(me, st_size, step, flip, -1)
        for rank in range(block_ref.shape[1]):
            items.append((got_refs[j], rank, jnp.clip(block_ref[owner, rank], 0, blocks - 1)))
    for first in range(0, len(items), GROUP):
        group = items[first : first + GROUP]
        scores = [nt(rq_ref[b], ref[rank, :, :DV]) for ref, rank, b in group]
        weights = [jnp.exp(score * DV ** (-0.5)).astype(BF16) for score in scores]
        reads = [
            jnp.dot(weight, ref[rank, :, DV:], preferred_element_type=F32)
            for weight, (ref, rank, _) in zip(weights, group)
        ]
        sums = [jnp.dot(weight, ones, preferred_element_type=F32) for weight in weights]
        for row_sum, read, (_, _, b) in zip(sums, reads, group):
            bottom_ref[b] += row_sum
            top_ref[b] += read


def early_kernel(offsets, st_size, me_ref, block_ref, rq_ref, *refs):
    got_refs, (top_ref, bottom_ref) = refs[:-2], refs[-2:]
    top_ref[...] = jnp.zeros_like(top_ref)
    bottom_ref[...] = jnp.zeros_like(bottom_ref)
    add_reads(offsets, st_size, me_ref, block_ref, rq_ref, got_refs, top_ref, bottom_ref)


def middle_kernel(offsets, st_size, me_ref, block_ref, rq_ref, top_in_ref, bottom_in_ref, *refs):
    got_refs, (top_ref, bottom_ref) = refs[:-2], refs[-2:]
    top_ref[...] = top_in_ref[...]
    bottom_ref[...] = bottom_in_ref[...]
    add_reads(offsets, st_size, me_ref, block_ref, rq_ref, got_refs, top_ref, bottom_ref)


def late_kernel(offsets, st_size, me_ref, block_ref, rq_ref, gla_ref, gate_ref, top_in_ref, bottom_in_ref, *refs):
    got_refs = refs[: len(offsets)]
    out_ref, square_ref, top_ref, bottom_ref = refs[len(offsets) :]
    top_ref[...] = top_in_ref[...]
    bottom_ref[...] = bottom_in_ref[...]
    add_reads(offsets, st_size, me_ref, block_ref, rq_ref, got_refs, top_ref, bottom_ref)
    blocks = rq_ref.shape[0]
    lane = lax.broadcasted_iota(jnp.int32, (BLK, DV), 1)
    sums = jnp.zeros((BLK, DV), F32)
    for b in range(blocks):
        combined = gla_ref[b] + gate_ref[b] * (top_ref[b] / bottom_ref[b])
        out_ref[b] = combined
        sums = jnp.where(lane == b, jnp.sum(combined * combined, axis=-1, keepdims=True), sums)
    rows = jnp.transpose(sums)[:blocks].reshape(1, blocks, 1, BLK)
    square_ref[...] = jnp.broadcast_to(rows, square_ref.shape)


def scale_kernel(square_ref, combined_ref, gain_ref, out_ref):
    total = jnp.sum(square_ref[...], axis=0)[:, 0, :]
    scale = lax.rsqrt(total / (HEADS * DV) + EPS)
    columns = jnp.transpose(scale)
    for b in range(total.shape[0]):
        at = slice(b * BLK, (b + 1) * BLK)
        out_ref[at] = (combined_ref[at] * columns[:, b : b + 1] * gain_ref[...]).astype(BF16)


VMEM = pl.BlockSpec(memory_space=pltpu.VMEM)
SMEM = pl.BlockSpec(memory_space=pltpu.SMEM)
ANY = pl.BlockSpec(memory_space=pl.ANY)


def whole(shape):
    return pl.BlockSpec(shape, lambda i: (0,) * len(shape))


def on_device(
    tokens,
    w_query,
    w_key,
    w_value,
    w_decay,
    decay_rate,
    block_scale,
    w_rquery,
    w_gate,
    w_rkey,
    w_rvalue,
    query_gain,
    key_gain,
    out_gain,
    store,
    passage_ids,
):
    length, width = tokens.shape
    blocks = length // BLK
    held, plen, _ = store.shape
    st_size = lax.axis_size("st")
    tp_size = lax.axis_size("tp")
    requests = passage_ids.shape[0] * passage_ids.shape[1]
    owners = min(st_size, requests // 2)
    most = requests // owners
    chips = st_size // 2
    me = lax.axis_index("st").astype(jnp.int32).reshape(1)

    wanted, block_of = pl.pallas_call(
        functools.partial(requests_kernel, held),
        out_shape=(
            jax.ShapeDtypeStruct((st_size, most), jnp.int32),
            jax.ShapeDtypeStruct((st_size, most), jnp.int32),
        ),
        in_specs=[VMEM],
        out_specs=(VMEM, VMEM),
        cost_estimate=pl.CostEstimate(flops=64 * held * plen * width * DV, bytes_accessed=0, transcendentals=0),
        compiler_params=pltpu.CompilerParams(vmem_limit_bytes=2 * MIB),
        name="requests",
    )(passage_ids.T)
    incoming = lax.all_to_all(wanted, "st", split_axis=0, concat_axis=0, tiled=True)

    made = pl.pallas_call(
        passages_kernel,
        out_shape=jax.ShapeDtypeStruct((held, plen, 2 * DV), BF16),
        in_specs=[VMEM, VMEM, VMEM, VMEM],
        out_specs=VMEM,
        scratch_shapes=[pltpu.VMEM((width, 2 * DV), BF16)],
        cost_estimate=pl.CostEstimate(
            flops=2 * held * plen * width * 2 * DV,
            bytes_accessed=2 * held * plen * (width + 2 * DV),
            transcendentals=0,
        ),
        compiler_params=pltpu.CompilerParams(vmem_limit_bytes=24 * MIB),
        name="passages",
    )(store, w_rkey, w_rvalue, key_gain.reshape(1, DV))

    half = chips // 2
    order = []
    for step in [*range(2, half + 1), 1]:
        ways = tuple(dict.fromkeys((step, chips - step)))
        order += [(way, flip) for flip in (0, 1) for way in ways]
    offsets = tuple(order + [(0, 1), (0, 0)])

    def pack(part):
        return pl.pallas_call(
            functools.partial(pack_kernel, part, st_size),
            out_shape=tuple(jax.ShapeDtypeStruct((most, plen, 2 * DV), BF16) for _ in part),
            in_specs=[SMEM, SMEM, VMEM],
            out_specs=tuple(VMEM for _ in part),
            compiler_params=pltpu.CompilerParams(vmem_limit_bytes=8 * MIB),
            name="pack",
        )(me, incoming, made)

    packed = [*pack(offsets[:LEAD]), *pack(offsets[LEAD:])]

    def sent(array, step, flip):
        pairs = [(2 * y + e, ((y + step) % chips) * 2 + (e + flip) % 2) for y in range(chips) for e in range(2)]
        return lax.ppermute(array, "st", pairs)

    got = []
    for j, offset in enumerate(offsets):
        got.append(packed[j] if offset == (0, 0) else sent(packed[j], *offset))

    rows = 4 * BLK
    gla, gate, read_query = pl.pallas_call(
        tokens_kernel,
        grid=(length // rows,),
        out_shape=(
            jax.ShapeDtypeStruct((length, DV), F32),
            jax.ShapeDtypeStruct((length, DV), F32),
            jax.ShapeDtypeStruct((length, DV), BF16),
        ),
        in_specs=[
            ANY,
            SMEM,
            pl.BlockSpec((rows, width), lambda i: (i, 0)),
            whole((DK, width)),
            whole((DK, width)),
            whole((DK, width)),
            whole((width, DV)),
            whole((width, DV)),
            whole((width, DV)),
            whole((1, DK)),
            whole((1, DV)),
        ],
        out_specs=(
            pl.BlockSpec((rows, DV), lambda i: (i, 0)),
            pl.BlockSpec((rows, DV), lambda i: (i, 0)),
            pl.BlockSpec((rows, DV), lambda i: (i, 0)),
        ),
        scratch_shapes=[
            pltpu.VMEM((3 * DK, width), BF16),
            pltpu.VMEM((width, 2 * DV), BF16),
            pltpu.VMEM((DV, DK), F32),
        ],
        cost_estimate=pl.CostEstimate(
            flops=20 * length * width * (3 * DK + 3 * DV), bytes_accessed=2 * length * width, transcendentals=0
        ),
        compiler_params=pltpu.CompilerParams(vmem_limit_bytes=51 * MIB),
        name="tokens",
    )(
        packed[-1],
        block_scale,
        tokens,
        w_query.T,
        w_key.T,
        w_decay.T,
        w_value,
        w_rquery,
        w_gate,
        decay_rate.reshape(1, DK),
        query_gain.reshape(1, DV),
    )

    blocked = (blocks, BLK, DV)
    read_query = read_query.reshape(blocked)
    sums = jax.ShapeDtypeStruct(blocked, F32)
    last = [j for j, (step, _) in enumerate(offsets) if min(step, chips - step) == 1]
    middle = [j for j, (step, _) in enumerate(offsets) if step == half]
    first = [j for j in range(len(offsets)) if j not in last + middle]
    top, bottom = pl.pallas_call(
        functools.partial(early_kernel, tuple(offsets[j] for j in first), st_size),
        out_shape=(sums, sums),
        in_specs=[SMEM, SMEM, VMEM] + [VMEM] * len(first),
        out_specs=(VMEM, VMEM),
        cost_estimate=pl.CostEstimate(
            flops=8 * len(first) * most * BLK * plen * DV, bytes_accessed=0, transcendentals=0
        ),
        compiler_params=pltpu.CompilerParams(vmem_limit_bytes=14 * MIB),
        name="early",
    )(me, block_of, read_query, *[got[j] for j in first])
    top, bottom = pl.pallas_call(
        functools.partial(middle_kernel, tuple(offsets[j] for j in middle), st_size),
        out_shape=(sums, sums),
        in_specs=[SMEM, SMEM] + [VMEM] * (3 + len(middle)),
        out_specs=(VMEM, VMEM),
        cost_estimate=pl.CostEstimate(
            flops=8 * len(middle) * most * BLK * plen * DV, bytes_accessed=0, transcendentals=0
        ),
        compiler_params=pltpu.CompilerParams(vmem_limit_bytes=14 * MIB),
        name="middle",
    )(me, block_of, read_query, top, bottom, *[got[j] for j in middle])
    combined, squares = pl.pallas_call(
        functools.partial(late_kernel, tuple(offsets[j] for j in last), st_size),
        out_shape=(sums, jax.ShapeDtypeStruct((tp_size, blocks, 1, BLK), F32)),
        in_specs=[SMEM, SMEM] + [VMEM] * (5 + len(last)),
        out_specs=(VMEM, VMEM),
        scratch_shapes=[pltpu.VMEM(blocked, F32), pltpu.VMEM(blocked, F32)],
        compiler_params=pltpu.CompilerParams(vmem_limit_bytes=14 * MIB),
        name="late",
    )(
        me,
        block_of,
        read_query,
        gla.reshape(blocked),
        gate.reshape(blocked),
        top,
        bottom,
        *[got[j] for j in last],
    )
    everyone = lax.all_to_all(squares, "tp", split_axis=0, concat_axis=0, tiled=True)

    return pl.pallas_call(
        scale_kernel,
        out_shape=jax.ShapeDtypeStruct((length, DV), BF16),
        in_specs=[VMEM, VMEM, VMEM],
        out_specs=VMEM,
        compiler_params=pltpu.CompilerParams(vmem_limit_bytes=8 * MIB),
        name="scale",
    )(everyone, combined.reshape(length, DV), out_gain.reshape(1, DV))


def solution(mesh):
    return jax.shard_map(
        on_device,
        mesh=mesh,
        in_specs=(
            P(("grp", "st"), None),
            P(None, "tp"),
            P(None, "tp"),
            P(None, "tp"),
            P(None, "tp"),
            P("tp"),
            P(("grp", "st")),
            P(None, "tp"),
            P(None, "tp"),
            P(None, "tp"),
            P(None, "tp"),
            P(),
            P(),
            P("tp"),
            P(("grp", "st"), None, None),
            P(("grp", "st"), None),
        ),
        out_specs=P(("grp", "st"), "tp"),
        check_vma=False,
    )
```

```python
import functools

import jax
import jax.numpy as jnp
from jax import lax
from jax.experimental import pallas as pl
from jax.experimental.pallas import tpu as pltpu
from jax.sharding import PartitionSpec as P

HEADS = 8
DK = 64
DV = 128
BLK = 128
NPASS = 4
PLEN = 128
EPS = 1e-06
PRECISE = lax.Precision.HIGHEST
F32 = jnp.float32
BF16 = jnp.bfloat16
MIB = 2**20
GROUP = 16
STRIDE = 4096


def nt(a, b, precision=None):
    return lax.dot_general(a, b, (((1,), (1,)), ((), ())), precision=precision, preferred_element_type=F32)


def head_norm(values, gain_row):
    return values * lax.rsqrt(jnp.mean(values * values, axis=-1, keepdims=True) + EPS) * gain_row


def requests_kernel(here, ids_ref, wanted_ref, block_ref):
    owners = wanted_ref.shape[0]
    passes, blocks = ids_ref.shape
    begin = here * lax.broadcasted_iota(jnp.int32, (owners, blocks), 0)
    column = lax.broadcasted_iota(jnp.int32, (owners, blocks), 1)
    low = jnp.full((owners, blocks), float(passes * blocks * STRIDE), F32)
    high = jnp.zeros((owners, blocks), F32)
    for j in range(passes):
        wanted = jnp.broadcast_to(ids_ref[j : j + 1, :], (owners, blocks))
        number = ((j * blocks + column) * STRIDE + wanted).astype(F32)
        asked = (wanted >= begin) & (wanted < begin + here)
        low = jnp.where(asked, jnp.minimum(low, number), low)
        high = jnp.where(asked, jnp.maximum(high, number), high)
    low = jnp.min(low, axis=1, keepdims=True).astype(jnp.int32)
    high = jnp.max(high, axis=1, keepdims=True).astype(jnp.int32)
    shape = wanted_ref.shape
    first = lax.broadcasted_iota(jnp.int32, shape, 1) == 0
    number = jnp.where(first, jnp.broadcast_to(low, shape), jnp.broadcast_to(high, shape))
    place = lax.shift_right_logical(number, STRIDE.bit_length() - 1)
    wanted_ref[...] = number - place * STRIDE - here * lax.broadcasted_iota(jnp.int32, shape, 0)
    block_ref[...] = lax.rem(place, blocks)


def passages_kernel(store_ref, wk_ref, wv_ref, gain_ref, out_ref, weight_ref):
    count, rows, width = store_ref.shape
    weight_ref[:, :DV] = wk_ref[...]
    weight_ref[:, DV:] = wv_ref[...]
    made = jnp.dot(store_ref[...].reshape(count * rows, width), weight_ref[...], preferred_element_type=F32)
    made = made.astype(BF16)
    keys = head_norm(made[:, :DV].astype(F32), gain_ref[...]).astype(BF16)
    out_ref[:, :, :DV] = keys.reshape(count, rows, DV)
    out_ref[:, :, DV:] = made[:, DV:].reshape(count, rows, DV)


def other_index(me, st_size, step, flip, sign):
    chips = st_size // 2
    return lax.rem(me // 2 + (step if sign > 0 else chips - step), chips) * 2 + lax.rem(me + flip, 2)


def pack_kernel(offsets, st_size, wanted_ref, made_ref, *out_refs):
    held = made_ref.shape[0]
    me = lax.axis_index("st")
    for j, (step, flip) in enumerate(offsets):
        reader = other_index(me, st_size, step, flip, 1)
        for rank in range(wanted_ref.shape[1]):
            row = jnp.clip(wanted_ref[reader, rank], 0, held - 1)
            out_refs[j][rank] = made_ref[row]


def tokens_kernel(
    after_ref,
    scale_ref,
    tok_ref,
    wq_ref,
    wk_ref,
    wd_ref,
    wv_ref,
    wr_ref,
    wg_ref,
    rate_ref,
    qgain_ref,
    gla_ref,
    gate_ref,
    rq_ref,
    narrow_ref,
    wide_ref,
    state_ref,
):
    step = pl.program_id(0)

    @pl.when(step == 0)
    def _():
        state_ref[...] = jnp.zeros_like(state_ref)
        narrow_ref[:DK] = wq_ref[...]
        narrow_ref[DK : 2 * DK] = wk_ref[...]
        narrow_ref[2 * DK :] = wd_ref[...]
        wide_ref[:, :DV] = wv_ref[...]
        wide_ref[:, DV:] = wr_ref[...]

    tokens = tok_ref[...]
    blocks = tokens.shape[0] // BLK
    narrow = nt(tokens, narrow_ref[...])
    wide = jnp.dot(tokens, wide_ref[...], preferred_element_type=F32)
    gate_ref[...] = jax.nn.sigmoid(jnp.dot(tokens, wg_ref[...], preferred_element_type=F32))
    rq_ref[...] = head_norm(wide[:, DV:], qgain_ref[...]).astype(BF16)
    row_id = lax.broadcasted_iota(jnp.int32, (BLK, BLK), 0)
    col_id = lax.broadcasted_iota(jnp.int32, (BLK, BLK), 1)
    causal = row_id >= col_id
    lower = causal.astype(F32)
    places = [slice(b * BLK, (b + 1) * BLK) for b in range(blocks)]
    totals = []
    for b, at in enumerate(places):
        log_decay = -2.0 * rate_ref[...] * jax.nn.sigmoid(narrow[at, 2 * DK :]) * scale_ref[step * blocks + b]
        totals.append(jnp.dot(lower, log_decay, precision=PRECISE, preferred_element_type=F32))
    parts = []
    for at, total in zip(places, totals):
        key = narrow[at, DK : 2 * DK]
        q_dec = narrow[at, :DK] * DK ** (-0.5) * jnp.exp(total)
        k_dec = key * jnp.exp(-total)
        scores = jnp.where(causal, nt(q_dec, k_dec, PRECISE), 0.0)
        parts.append((q_dec, scores, key * jnp.exp(total[BLK - 1 :] - total)))
    inner = []
    for at, (_, scores, k_end) in zip(places, parts):
        value = wide[at, :DV]
        within = jnp.dot(scores, value, precision=PRECISE, preferred_element_type=F32)
        update = lax.dot_general(
            value, k_end, (((0,), (0,)), ((), ())), precision=PRECISE, preferred_element_type=F32
        )
        inner.append((within, update))
    for at, total, (q_dec, _, _), (within, update) in zip(places, totals, parts, inner):
        gla_ref[at] = within + nt(q_dec, state_ref[...], PRECISE)
        state_ref[...] = state_ref[...] * jnp.exp(total[BLK - 1 :]) + update


def add_reads(offsets, st_size, block_ref, rq_ref, got_refs, top_ref, bottom_ref):
    ones = jnp.ones((PLEN, DV), BF16)
    blocks = rq_ref.shape[0]
    me = lax.axis_index("st")
    items = []
    for j, (step, flip) in enumerate(offsets):
        owner = other_index(me, st_size, step, flip, -1)
        for rank in range(block_ref.shape[1]):
            items.append((got_refs[j], rank, jnp.clip(block_ref[owner, rank], 0, blocks - 1)))
    for first in range(0, len(items), GROUP):
        group = items[first : first + GROUP]
        scores = [nt(rq_ref[b], ref[rank, :, :DV]) for ref, rank, b in group]
        weights = [jnp.exp(score * DV ** (-0.5)).astype(BF16) for score in scores]
        reads = [
            jnp.dot(weight, ref[rank, :, DV:], preferred_element_type=F32)
            for weight, (ref, rank, _) in zip(weights, group)
        ]
        sums = [jnp.dot(weight, ones, preferred_element_type=F32) for weight in weights]
        for row_sum, read, (_, _, b) in zip(sums, reads, group):
            bottom_ref[b] += row_sum
            top_ref[b] += read


def early_kernel(offsets, st_size, block_ref, rq_ref, *refs):
    got_refs, (top_ref, bottom_ref) = refs[:-2], refs[-2:]
    top_ref[...] = jnp.zeros_like(top_ref)
    bottom_ref[...] = jnp.zeros_like(bottom_ref)
    add_reads(offsets, st_size, block_ref, rq_ref, got_refs, top_ref, bottom_ref)


def middle_kernel(offsets, st_size, block_ref, rq_ref, top_in_ref, bottom_in_ref, *refs):
    got_refs, (top_ref, bottom_ref) = refs[:-2], refs[-2:]
    top_ref[...] = top_in_ref[...]
    bottom_ref[...] = bottom_in_ref[...]
    add_reads(offsets, st_size, block_ref, rq_ref, got_refs, top_ref, bottom_ref)


def late_kernel(offsets, st_size, block_ref, rq_ref, gla_ref, gate_ref, top_in_ref, bottom_in_ref, *refs):
    got_refs = refs[: len(offsets)]
    out_ref, square_ref, top_ref, bottom_ref = refs[len(offsets) :]
    top_ref[...] = top_in_ref[...]
    bottom_ref[...] = bottom_in_ref[...]
    add_reads(offsets, st_size, block_ref, rq_ref, got_refs, top_ref, bottom_ref)
    blocks = rq_ref.shape[0]
    lane = lax.broadcasted_iota(jnp.int32, (BLK, DV), 1)
    sums = jnp.zeros((BLK, DV), F32)
    for b in range(blocks):
        combined = gla_ref[b] + gate_ref[b] * (top_ref[b] / bottom_ref[b])
        out_ref[b] = combined
        sums = jnp.where(lane == b, jnp.sum(combined * combined, axis=-1, keepdims=True), sums)
    rows = jnp.transpose(sums)[:blocks].reshape(1, blocks, 1, BLK)
    square_ref[...] = jnp.broadcast_to(rows, square_ref.shape)


def scale_kernel(square_ref, combined_ref, gain_ref, out_ref):
    total = jnp.sum(square_ref[...], axis=0)[:, 0, :]
    scale = lax.rsqrt(total / (HEADS * DV) + EPS)
    columns = jnp.transpose(scale)
    for b in range(total.shape[0]):
        at = slice(b * BLK, (b + 1) * BLK)
        out_ref[at] = (combined_ref[at] * columns[:, b : b + 1] * gain_ref[...]).astype(BF16)


VMEM = pl.BlockSpec(memory_space=pltpu.VMEM)
SMEM = pl.BlockSpec(memory_space=pltpu.SMEM)
ANY = pl.BlockSpec(memory_space=pl.ANY)


def whole(shape):
    return pl.BlockSpec(shape, lambda i: (0,) * len(shape))


def on_device(
    tokens,
    w_query,
    w_key,
    w_value,
    w_decay,
    decay_rate,
    block_scale,
    w_rquery,
    w_gate,
    w_rkey,
    w_rvalue,
    query_gain,
    key_gain,
    out_gain,
    store,
    passage_ids,
):
    length, width = tokens.shape
    blocks = length // BLK
    held, plen, _ = store.shape
    st_size = lax.axis_size("st")
    tp_size = lax.axis_size("tp")
    requests = passage_ids.shape[0] * passage_ids.shape[1]
    owners = min(st_size, requests // 2)
    most = requests // owners
    chips = st_size // 2

    wanted, block_of = pl.pallas_call(
        functools.partial(requests_kernel, held),
        out_shape=(
            jax.ShapeDtypeStruct((st_size, most), jnp.int32),
            jax.ShapeDtypeStruct((st_size, most), jnp.int32),
        ),
        in_specs=[VMEM],
        out_specs=(VMEM, VMEM),
        cost_estimate=pl.CostEstimate(flops=64 * held * plen * width * DV, bytes_accessed=0, transcendentals=0),
        compiler_params=pltpu.CompilerParams(vmem_limit_bytes=2 * MIB),
        name="requests",
    )(passage_ids.T)
    incoming = lax.all_to_all(wanted, "st", split_axis=0, concat_axis=0, tiled=True)

    made = pl.pallas_call(
        passages_kernel,
        out_shape=jax.ShapeDtypeStruct((held, plen, 2 * DV), BF16),
        in_specs=[VMEM, VMEM, VMEM, VMEM],
        out_specs=VMEM,
        scratch_shapes=[pltpu.VMEM((width, 2 * DV), BF16)],
        cost_estimate=pl.CostEstimate(
            flops=2 * held * plen * width * 2 * DV,
            bytes_accessed=2 * held * plen * (width + 2 * DV),
            transcendentals=0,
        ),
        compiler_params=pltpu.CompilerParams(vmem_limit_bytes=24 * MIB),
        name="passages",
    )(store, w_rkey, w_rvalue, key_gain.reshape(1, DV))

    half = chips // 2
    order = []
    for step in [*range(2, half + 1), 1]:
        ways = tuple(dict.fromkeys((step, chips - step)))
        order += [(way, flip) for flip in (0, 1) for way in ways]
    offsets = tuple(order + [(0, 1), (0, 0)])
    packed = pl.pallas_call(
        functools.partial(pack_kernel, offsets, st_size),
        out_shape=tuple(jax.ShapeDtypeStruct((most, plen, 2 * DV), BF16) for _ in offsets),
        in_specs=[SMEM, VMEM],
        out_specs=tuple(VMEM for _ in offsets),
        compiler_params=pltpu.CompilerParams(vmem_limit_bytes=8 * MIB),
        name="pack",
    )(incoming, made)

    def sent(array, step, flip):
        pairs = [(2 * y + e, ((y + step) % chips) * 2 + (e + flip) % 2) for y in range(chips) for e in range(2)]
        return lax.ppermute(array, "st", pairs)

    got = [packed[j] if o == (0, 0) else sent(packed[j], *o) for j, o in enumerate(offsets)]

    rows = 4 * BLK
    gla, gate, read_query = pl.pallas_call(
        tokens_kernel,
        grid=(length // rows,),
        out_shape=(
            jax.ShapeDtypeStruct((length, DV), F32),
            jax.ShapeDtypeStruct((length, DV), F32),
            jax.ShapeDtypeStruct((length, DV), BF16),
        ),
        in_specs=[
            ANY,
            SMEM,
            pl.BlockSpec((rows, width), lambda i: (i, 0)),
            whole((DK, width)),
            whole((DK, width)),
            whole((DK, width)),
            whole((width, DV)),
            whole((width, DV)),
            whole((width, DV)),
            whole((1, DK)),
            whole((1, DV)),
        ],
        out_specs=(
            pl.BlockSpec((rows, DV), lambda i: (i, 0)),
            pl.BlockSpec((rows, DV), lambda i: (i, 0)),
            pl.BlockSpec((rows, DV), lambda i: (i, 0)),
        ),
        scratch_shapes=[
            pltpu.VMEM((3 * DK, width), BF16),
            pltpu.VMEM((width, 2 * DV), BF16),
            pltpu.VMEM((DV, DK), F32),
        ],
        cost_estimate=pl.CostEstimate(
            flops=20 * length * width * (3 * DK + 3 * DV), bytes_accessed=2 * length * width, transcendentals=0
        ),
        compiler_params=pltpu.CompilerParams(vmem_limit_bytes=51 * MIB),
        name="tokens",
    )(
        packed[-1],
        block_scale,
        tokens,
        w_query.T,
        w_key.T,
        w_decay.T,
        w_value,
        w_rquery,
        w_gate,
        decay_rate.reshape(1, DK),
        query_gain.reshape(1, DV),
    )

    blocked = (blocks, BLK, DV)
    read_query = read_query.reshape(blocked)
    sums = jax.ShapeDtypeStruct(blocked, F32)
    last = [j for j, (step, _) in enumerate(offsets) if min(step, chips - step) == 1]
    middle = [j for j, (step, _) in enumerate(offsets) if step == half]
    first = [j for j in range(len(offsets)) if j not in last + middle]
    top, bottom = pl.pallas_call(
        functools.partial(early_kernel, tuple(offsets[j] for j in first), st_size),
        out_shape=(sums, sums),
        in_specs=[SMEM, VMEM] + [VMEM] * len(first),
        out_specs=(VMEM, VMEM),
        cost_estimate=pl.CostEstimate(
            flops=8 * len(first) * most * BLK * plen * DV, bytes_accessed=0, transcendentals=0
        ),
        compiler_params=pltpu.CompilerParams(vmem_limit_bytes=14 * MIB),
        name="early",
    )(block_of, read_query, *[got[j] for j in first])
    top, bottom = pl.pallas_call(
        functools.partial(middle_kernel, tuple(offsets[j] for j in middle), st_size),
        out_shape=(sums, sums),
        in_specs=[SMEM] + [VMEM] * (3 + len(middle)),
        out_specs=(VMEM, VMEM),
        cost_estimate=pl.CostEstimate(
            flops=8 * len(middle) * most * BLK * plen * DV, bytes_accessed=0, transcendentals=0
        ),
        compiler_params=pltpu.CompilerParams(vmem_limit_bytes=14 * MIB),
        name="middle",
    )(block_of, read_query, top, bottom, *[got[j] for j in middle])
    combined, squares = pl.pallas_call(
        functools.partial(late_kernel, tuple(offsets[j] for j in last), st_size),
        out_shape=(sums, jax.ShapeDtypeStruct((tp_size, blocks, 1, BLK), F32)),
        in_specs=[SMEM] + [VMEM] * (5 + len(last)),
        out_specs=(VMEM, VMEM),
        scratch_shapes=[pltpu.VMEM(blocked, F32), pltpu.VMEM(blocked, F32)],
        compiler_params=pltpu.CompilerParams(vmem_limit_bytes=14 * MIB),
        name="late",
    )(
        block_of,
        read_query,
        gla.reshape(blocked),
        gate.reshape(blocked),
        top,
        bottom,
        *[got[j] for j in last],
    )
    everyone = lax.all_to_all(squares, "tp", split_axis=0, concat_axis=0, tiled=True)

    return pl.pallas_call(
        scale_kernel,
        out_shape=jax.ShapeDtypeStruct((length, DV), BF16),
        in_specs=[VMEM, VMEM, VMEM],
        out_specs=VMEM,
        compiler_params=pltpu.CompilerParams(vmem_limit_bytes=8 * MIB),
        name="scale",
    )(everyone, combined.reshape(length, DV), out_gain.reshape(1, DV))


def solution(mesh):
    return jax.shard_map(
        on_device,
        mesh=mesh,
        in_specs=(
            P(("grp", "st"), None),
            P(None, "tp"),
            P(None, "tp"),
            P(None, "tp"),
            P(None, "tp"),
            P("tp"),
            P(("grp", "st")),
            P(None, "tp"),
            P(None, "tp"),
            P(None, "tp"),
            P(None, "tp"),
            P(),
            P(),
            P("tp"),
            P(("grp", "st"), None, None),
            P(("grp", "st"), None),
        ),
        out_specs=P(("grp", "st"), "tp"),
        check_vma=False,
    )
```

```python
import functools

import jax
import jax.numpy as jnp
from jax import lax
from jax.experimental import pallas as pl
from jax.experimental.pallas import tpu as pltpu
from jax.sharding import PartitionSpec as P

HEADS = 8
DK = 64
DV = 128
BLK = 128
NPASS = 4
PLEN = 128
EPS = 1e-06
PRECISE = lax.Precision.HIGHEST
F32 = jnp.float32
BF16 = jnp.bfloat16
MIB = 2**20
GROUP = 16
STRIDE = 4096


def nt(a, b, precision=None):
    return lax.dot_general(a, b, (((1,), (1,)), ((), ())), precision=precision, preferred_element_type=F32)


def head_norm(values, gain_row):
    return values * lax.rsqrt(jnp.mean(values * values, axis=-1, keepdims=True) + EPS) * gain_row


def requests_kernel(here, ids_ref, wanted_ref, block_ref):
    owners = wanted_ref.shape[0]
    passes, blocks = ids_ref.shape
    begin = here * lax.broadcasted_iota(jnp.int32, (owners, blocks), 0)
    column = lax.broadcasted_iota(jnp.int32, (owners, blocks), 1)
    low = jnp.full((owners, blocks), float(passes * blocks * STRIDE), F32)
    high = jnp.zeros((owners, blocks), F32)
    for j in range(passes):
        wanted = jnp.broadcast_to(ids_ref[j : j + 1, :], (owners, blocks))
        number = ((j * blocks + column) * STRIDE + wanted).astype(F32)
        asked = (wanted >= begin) & (wanted < begin + here)
        low = jnp.where(asked, jnp.minimum(low, number), low)
        high = jnp.where(asked, jnp.maximum(high, number), high)
    low = jnp.min(low, axis=1, keepdims=True).astype(jnp.int32)
    high = jnp.max(high, axis=1, keepdims=True).astype(jnp.int32)
    shape = wanted_ref.shape
    first = lax.broadcasted_iota(jnp.int32, shape, 1) == 0
    number = jnp.where(first, jnp.broadcast_to(low, shape), jnp.broadcast_to(high, shape))
    place = lax.shift_right_logical(number, STRIDE.bit_length() - 1)
    wanted_ref[...] = number - place * STRIDE - here * lax.broadcasted_iota(jnp.int32, shape, 0)
    block_ref[...] = lax.rem(place, blocks)


def passages_kernel(store_ref, wk_ref, wv_ref, gain_ref, out_ref, weight_ref):
    count, rows, width = store_ref.shape
    weight_ref[:, :DV] = wk_ref[...]
    weight_ref[:, DV:] = wv_ref[...]
    made = jnp.dot(store_ref[...].reshape(count * rows, width), weight_ref[...], preferred_element_type=F32)
    made = made.astype(BF16)
    keys = head_norm(made[:, :DV].astype(F32), gain_ref[...]).astype(BF16)
    out_ref[:, :, :DV] = keys.reshape(count, rows, DV)
    out_ref[:, :, DV:] = made[:, DV:].reshape(count, rows, DV)


def other_index(me, st_size, step, flip, sign):
    chips = st_size // 2
    other_core = lax.rem(me + flip, 2)
    sender_core = lax.rem(me, 2) if sign > 0 else other_core
    shift = jnp.where(sender_core == 0, step, (chips - step) % chips)
    return lax.rem(me // 2 + (shift if sign > 0 else chips - shift), chips) * 2 + other_core


def pack_kernel(offsets, st_size, wanted_ref, made_ref, *out_refs):
    held = made_ref.shape[0]
    me = lax.axis_index("st")
    for j, (step, flip) in enumerate(offsets):
        reader = other_index(me, st_size, step, flip, 1)
        for rank in range(wanted_ref.shape[1]):
            row = jnp.clip(wanted_ref[reader, rank], 0, held - 1)
            out_refs[j][rank] = made_ref[row]


def tokens_kernel(
    after_ref,
    scale_ref,
    tok_ref,
    wq_ref,
    wk_ref,
    wd_ref,
    wv_ref,
    wr_ref,
    wg_ref,
    rate_ref,
    qgain_ref,
    gla_ref,
    gate_ref,
    rq_ref,
    narrow_ref,
    wide_ref,
    state_ref,
):
    step = pl.program_id(0)

    @pl.when(step == 0)
    def _():
        state_ref[...] = jnp.zeros_like(state_ref)
        narrow_ref[:DK] = wq_ref[...]
        narrow_ref[DK : 2 * DK] = wk_ref[...]
        narrow_ref[2 * DK :] = wd_ref[...]
        wide_ref[:, :DV] = wv_ref[...]
        wide_ref[:, DV:] = wr_ref[...]

    tokens = tok_ref[...]
    blocks = tokens.shape[0] // BLK
    narrow = nt(tokens, narrow_ref[...])
    wide = jnp.dot(tokens, wide_ref[...], preferred_element_type=F32)
    gate_ref[...] = jax.nn.sigmoid(jnp.dot(tokens, wg_ref[...], preferred_element_type=F32))
    rq_ref[...] = head_norm(wide[:, DV:], qgain_ref[...]).astype(BF16)
    row_id = lax.broadcasted_iota(jnp.int32, (BLK, BLK), 0)
    col_id = lax.broadcasted_iota(jnp.int32, (BLK, BLK), 1)
    causal = row_id >= col_id
    lower = causal.astype(F32)
    places = [slice(b * BLK, (b + 1) * BLK) for b in range(blocks)]
    totals = []
    for b, at in enumerate(places):
        log_decay = -2.0 * rate_ref[...] * jax.nn.sigmoid(narrow[at, 2 * DK :]) * scale_ref[step * blocks + b]
        totals.append(jnp.dot(lower, log_decay, precision=PRECISE, preferred_element_type=F32))
    parts = []
    for at, total in zip(places, totals):
        key = narrow[at, DK : 2 * DK]
        q_dec = narrow[at, :DK] * DK ** (-0.5) * jnp.exp(total)
        k_dec = key * jnp.exp(-total)
        scores = jnp.where(causal, nt(q_dec, k_dec, PRECISE), 0.0)
        parts.append((q_dec, scores, key * jnp.exp(total[BLK - 1 :] - total)))
    inner = []
    for at, (_, scores, k_end) in zip(places, parts):
        value = wide[at, :DV]
        within = jnp.dot(scores, value, precision=PRECISE, preferred_element_type=F32)
        update = lax.dot_general(
            value, k_end, (((0,), (0,)), ((), ())), precision=PRECISE, preferred_element_type=F32
        )
        inner.append((within, update))
    for at, total, (q_dec, _, _), (within, update) in zip(places, totals, parts, inner):
        gla_ref[at] = within + nt(q_dec, state_ref[...], PRECISE)
        state_ref[...] = state_ref[...] * jnp.exp(total[BLK - 1 :]) + update


def add_reads(offsets, st_size, block_ref, rq_ref, got_refs, top_ref, bottom_ref):
    ones = jnp.ones((PLEN, DV), BF16)
    blocks = rq_ref.shape[0]
    me = lax.axis_index("st")
    items = []
    for j, (step, flip) in enumerate(offsets):
        owner = other_index(me, st_size, step, flip, -1)
        for rank in range(block_ref.shape[1]):
            items.append((got_refs[j], rank, jnp.clip(block_ref[owner, rank], 0, blocks - 1)))
    for first in range(0, len(items), GROUP):
        group = items[first : first + GROUP]
        scores = [nt(rq_ref[b], ref[rank, :, :DV]) for ref, rank, b in group]
        weights = [jnp.exp(score * DV ** (-0.5)).astype(BF16) for score in scores]
        reads = [
            jnp.dot(weight, ref[rank, :, DV:], preferred_element_type=F32)
            for weight, (ref, rank, _) in zip(weights, group)
        ]
        sums = [jnp.dot(weight, ones, preferred_element_type=F32) for weight in weights]
        for row_sum, read, (_, _, b) in zip(sums, reads, group):
            bottom_ref[b] += row_sum
            top_ref[b] += read


def early_kernel(offsets, st_size, block_ref, rq_ref, *refs):
    got_refs, (top_ref, bottom_ref) = refs[:-2], refs[-2:]
    top_ref[...] = jnp.zeros_like(top_ref)
    bottom_ref[...] = jnp.zeros_like(bottom_ref)
    add_reads(offsets, st_size, block_ref, rq_ref, got_refs, top_ref, bottom_ref)


def middle_kernel(offsets, st_size, block_ref, rq_ref, top_in_ref, bottom_in_ref, *refs):
    got_refs, (top_ref, bottom_ref) = refs[:-2], refs[-2:]
    top_ref[...] = top_in_ref[...]
    bottom_ref[...] = bottom_in_ref[...]
    add_reads(offsets, st_size, block_ref, rq_ref, got_refs, top_ref, bottom_ref)


def late_kernel(offsets, st_size, block_ref, rq_ref, gla_ref, gate_ref, top_in_ref, bottom_in_ref, *refs):
    got_refs = refs[: len(offsets)]
    out_ref, square_ref, top_ref, bottom_ref = refs[len(offsets) :]
    top_ref[...] = top_in_ref[...]
    bottom_ref[...] = bottom_in_ref[...]
    add_reads(offsets, st_size, block_ref, rq_ref, got_refs, top_ref, bottom_ref)
    blocks = rq_ref.shape[0]
    lane = lax.broadcasted_iota(jnp.int32, (BLK, DV), 1)
    sums = jnp.zeros((BLK, DV), F32)
    for b in range(blocks):
        combined = gla_ref[b] + gate_ref[b] * (top_ref[b] / bottom_ref[b])
        out_ref[b] = combined
        sums = jnp.where(lane == b, jnp.sum(combined * combined, axis=-1, keepdims=True), sums)
    rows = jnp.transpose(sums)[:blocks].reshape(1, blocks, 1, BLK)
    square_ref[...] = jnp.broadcast_to(rows, square_ref.shape)


def scale_kernel(square_ref, combined_ref, gain_ref, out_ref):
    total = jnp.sum(square_ref[...], axis=0)[:, 0, :]
    scale = lax.rsqrt(total / (HEADS * DV) + EPS)
    columns = jnp.transpose(scale)
    for b in range(total.shape[0]):
        at = slice(b * BLK, (b + 1) * BLK)
        out_ref[at] = (combined_ref[at] * columns[:, b : b + 1] * gain_ref[...]).astype(BF16)


VMEM = pl.BlockSpec(memory_space=pltpu.VMEM)
SMEM = pl.BlockSpec(memory_space=pltpu.SMEM)
ANY = pl.BlockSpec(memory_space=pl.ANY)


def whole(shape):
    return pl.BlockSpec(shape, lambda i: (0,) * len(shape))


def on_device(
    tokens,
    w_query,
    w_key,
    w_value,
    w_decay,
    decay_rate,
    block_scale,
    w_rquery,
    w_gate,
    w_rkey,
    w_rvalue,
    query_gain,
    key_gain,
    out_gain,
    store,
    passage_ids,
):
    length, width = tokens.shape
    blocks = length // BLK
    held, plen, _ = store.shape
    st_size = lax.axis_size("st")
    tp_size = lax.axis_size("tp")
    requests = passage_ids.shape[0] * passage_ids.shape[1]
    owners = min(st_size, requests // 2)
    most = requests // owners
    chips = st_size // 2

    wanted, block_of = pl.pallas_call(
        functools.partial(requests_kernel, held),
        out_shape=(
            jax.ShapeDtypeStruct((st_size, most), jnp.int32),
            jax.ShapeDtypeStruct((st_size, most), jnp.int32),
        ),
        in_specs=[VMEM],
        out_specs=(VMEM, VMEM),
        cost_estimate=pl.CostEstimate(flops=64 * held * plen * width * DV, bytes_accessed=0, transcendentals=0),
        compiler_params=pltpu.CompilerParams(vmem_limit_bytes=2 * MIB),
        name="requests",
    )(passage_ids.T)
    incoming = lax.all_to_all(wanted, "st", split_axis=0, concat_axis=0, tiled=True)

    made = pl.pallas_call(
        passages_kernel,
        out_shape=jax.ShapeDtypeStruct((held, plen, 2 * DV), BF16),
        in_specs=[VMEM, VMEM, VMEM, VMEM],
        out_specs=VMEM,
        scratch_shapes=[pltpu.VMEM((width, 2 * DV), BF16)],
        cost_estimate=pl.CostEstimate(
            flops=2 * held * plen * width * 2 * DV,
            bytes_accessed=2 * held * plen * (width + 2 * DV),
            transcendentals=0,
        ),
        compiler_params=pltpu.CompilerParams(vmem_limit_bytes=24 * MIB),
        name="passages",
    )(store, w_rkey, w_rvalue, key_gain.reshape(1, DV))

    half = chips // 2
    order = []
    for step in [*range(2, half + 1), 1]:
        ways = tuple(dict.fromkeys((step, chips - step)))
        order += [(way, flip) for flip in (0, 1) for way in ways]
    offsets = tuple(order + [(0, 1), (0, 0)])
    packed = pl.pallas_call(
        functools.partial(pack_kernel, offsets, st_size),
        out_shape=tuple(jax.ShapeDtypeStruct((most, plen, 2 * DV), BF16) for _ in offsets),
        in_specs=[SMEM, VMEM],
        out_specs=tuple(VMEM for _ in offsets),
        compiler_params=pltpu.CompilerParams(vmem_limit_bytes=8 * MIB),
        name="pack",
    )(incoming, made)

    def sent(array, step, flip):
        pairs = [
            (2 * y + e, ((y + (step, -step)[e]) % chips) * 2 + (e + flip) % 2) for y in range(chips) for e in range(2)
        ]
        return lax.ppermute(array, "st", pairs)

    got = [packed[j] if o == (0, 0) else sent(packed[j], *o) for j, o in enumerate(offsets)]

    rows = 4 * BLK
    gla, gate, read_query = pl.pallas_call(
        tokens_kernel,
        grid=(length // rows,),
        out_shape=(
            jax.ShapeDtypeStruct((length, DV), F32),
            jax.ShapeDtypeStruct((length, DV), F32),
            jax.ShapeDtypeStruct((length, DV), BF16),
        ),
        in_specs=[
            ANY,
            SMEM,
            pl.BlockSpec((rows, width), lambda i: (i, 0)),
            whole((DK, width)),
            whole((DK, width)),
            whole((DK, width)),
            whole((width, DV)),
            whole((width, DV)),
            whole((width, DV)),
            whole((1, DK)),
            whole((1, DV)),
        ],
        out_specs=(
            pl.BlockSpec((rows, DV), lambda i: (i, 0)),
            pl.BlockSpec((rows, DV), lambda i: (i, 0)),
            pl.BlockSpec((rows, DV), lambda i: (i, 0)),
        ),
        scratch_shapes=[
            pltpu.VMEM((3 * DK, width), BF16),
            pltpu.VMEM((width, 2 * DV), BF16),
            pltpu.VMEM((DV, DK), F32),
        ],
        cost_estimate=pl.CostEstimate(
            flops=20 * length * width * (3 * DK + 3 * DV), bytes_accessed=2 * length * width, transcendentals=0
        ),
        compiler_params=pltpu.CompilerParams(vmem_limit_bytes=51 * MIB),
        name="tokens",
    )(
        packed[-1],
        block_scale,
        tokens,
        w_query.T,
        w_key.T,
        w_decay.T,
        w_value,
        w_rquery,
        w_gate,
        decay_rate.reshape(1, DK),
        query_gain.reshape(1, DV),
    )

    blocked = (blocks, BLK, DV)
    read_query = read_query.reshape(blocked)
    sums = jax.ShapeDtypeStruct(blocked, F32)
    last = [j for j, (step, _) in enumerate(offsets) if min(step, chips - step) == 1]
    middle = [j for j, (step, _) in enumerate(offsets) if step == half]
    first = [j for j in range(len(offsets)) if j not in last + middle]
    top, bottom = pl.pallas_call(
        functools.partial(early_kernel, tuple(offsets[j] for j in first), st_size),
        out_shape=(sums, sums),
        in_specs=[SMEM, VMEM] + [VMEM] * len(first),
        out_specs=(VMEM, VMEM),
        cost_estimate=pl.CostEstimate(
            flops=8 * len(first) * most * BLK * plen * DV, bytes_accessed=0, transcendentals=0
        ),
        compiler_params=pltpu.CompilerParams(vmem_limit_bytes=14 * MIB),
        name="early",
    )(block_of, read_query, *[got[j] for j in first])
    top, bottom = pl.pallas_call(
        functools.partial(middle_kernel, tuple(offsets[j] for j in middle), st_size),
        out_shape=(sums, sums),
        in_specs=[SMEM] + [VMEM] * (3 + len(middle)),
        out_specs=(VMEM, VMEM),
        cost_estimate=pl.CostEstimate(
            flops=8 * len(middle) * most * BLK * plen * DV, bytes_accessed=0, transcendentals=0
        ),
        compiler_params=pltpu.CompilerParams(vmem_limit_bytes=14 * MIB),
        name="middle",
    )(block_of, read_query, top, bottom, *[got[j] for j in middle])
    combined, squares = pl.pallas_call(
        functools.partial(late_kernel, tuple(offsets[j] for j in last), st_size),
        out_shape=(sums, jax.ShapeDtypeStruct((tp_size, blocks, 1, BLK), F32)),
        in_specs=[SMEM] + [VMEM] * (5 + len(last)),
        out_specs=(VMEM, VMEM),
        scratch_shapes=[pltpu.VMEM(blocked, F32), pltpu.VMEM(blocked, F32)],
        compiler_params=pltpu.CompilerParams(vmem_limit_bytes=14 * MIB),
        name="late",
    )(
        block_of,
        read_query,
        gla.reshape(blocked),
        gate.reshape(blocked),
        top,
        bottom,
        *[got[j] for j in last],
    )
    everyone = lax.all_to_all(squares, "tp", split_axis=0, concat_axis=0, tiled=True)

    return pl.pallas_call(
        scale_kernel,
        out_shape=jax.ShapeDtypeStruct((length, DV), BF16),
        in_specs=[VMEM, VMEM, VMEM],
        out_specs=VMEM,
        compiler_params=pltpu.CompilerParams(vmem_limit_bytes=8 * MIB),
        name="scale",
    )(everyone, combined.reshape(length, DV), out_gain.reshape(1, DV))


def solution(mesh):
    return jax.shard_map(
        on_device,
        mesh=mesh,
        in_specs=(
            P(("grp", "st"), None),
            P(None, "tp"),
            P(None, "tp"),
            P(None, "tp"),
            P(None, "tp"),
            P("tp"),
            P(("grp", "st")),
            P(None, "tp"),
            P(None, "tp"),
            P(None, "tp"),
            P(None, "tp"),
            P(),
            P(),
            P("tp"),
            P(("grp", "st"), None, None),
            P(("grp", "st"), None),
        ),
        out_specs=P(("grp", "st"), "tp"),
        check_vma=False,
    )
```

```python
import functools

import jax
import jax.numpy as jnp
from jax import lax
from jax.experimental import pallas as pl
from jax.experimental.pallas import tpu as pltpu
from jax.sharding import PartitionSpec as P

HEADS = 8
DK = 64
DV = 128
BLK = 128
NPASS = 4
PLEN = 128
EPS = 1e-06
PRECISE = lax.Precision.HIGHEST
F32 = jnp.float32
BF16 = jnp.bfloat16
MIB = 2**20
GROUP = 16
STRIDE = 4096


def nt(a, b, precision=None):
    return lax.dot_general(a, b, (((1,), (1,)), ((), ())), precision=precision, preferred_element_type=F32)


def head_norm(values, gain_row):
    return values * lax.rsqrt(jnp.mean(values * values, axis=-1, keepdims=True) + EPS) * gain_row


def requests_kernel(here, ids_ref, wanted_ref, block_ref):
    owners = wanted_ref.shape[0]
    passes, blocks = ids_ref.shape
    begin = here * lax.broadcasted_iota(jnp.int32, (owners, blocks), 0)
    column = lax.broadcasted_iota(jnp.int32, (owners, blocks), 1)
    low = jnp.full((owners, blocks), float(passes * blocks * STRIDE), F32)
    high = jnp.zeros((owners, blocks), F32)
    for j in range(passes):
        wanted = jnp.broadcast_to(ids_ref[j : j + 1, :], (owners, blocks))
        number = ((j * blocks + column) * STRIDE + wanted).astype(F32)
        asked = (wanted >= begin) & (wanted < begin + here)
        low = jnp.where(asked, jnp.minimum(low, number), low)
        high = jnp.where(asked, jnp.maximum(high, number), high)
    low = jnp.min(low, axis=1, keepdims=True).astype(jnp.int32)
    high = jnp.max(high, axis=1, keepdims=True).astype(jnp.int32)
    shape = wanted_ref.shape
    first = lax.broadcasted_iota(jnp.int32, shape, 1) == 0
    number = jnp.where(first, jnp.broadcast_to(low, shape), jnp.broadcast_to(high, shape))
    place = lax.shift_right_logical(number, STRIDE.bit_length() - 1)
    wanted_ref[...] = number - place * STRIDE - here * lax.broadcasted_iota(jnp.int32, shape, 0)
    block_ref[...] = lax.rem(place, blocks)


def passages_kernel(store_ref, wk_ref, wv_ref, gain_ref, out_ref, weight_ref):
    count, rows, width = store_ref.shape
    weight_ref[:, :DV] = wk_ref[...]
    weight_ref[:, DV:] = wv_ref[...]
    made = jnp.dot(store_ref[...].reshape(count * rows, width), weight_ref[...], preferred_element_type=F32)
    made = made.astype(BF16)
    keys = head_norm(made[:, :DV].astype(F32), gain_ref[...]).astype(BF16)
    out_ref[:, :, :DV] = keys.reshape(count, rows, DV)
    out_ref[:, :, DV:] = made[:, DV:].reshape(count, rows, DV)


def other_index(me, st_size, step, flip, sign):
    chips = st_size // 2
    other_core = lax.rem(me + flip, 2)
    sender_core = lax.rem(me, 2) if sign > 0 else other_core
    shift = jnp.where(sender_core == 0, step, (chips - step) % chips)
    return lax.rem(me // 2 + (shift if sign > 0 else chips - shift), chips) * 2 + other_core


def pack_kernel(offsets, st_size, wanted_ref, made_ref, *out_refs):
    held = made_ref.shape[0]
    me = lax.axis_index("st")
    for j, (step, flip) in enumerate(offsets):
        reader = other_index(me, st_size, step, flip, 1)
        for rank in range(wanted_ref.shape[1]):
            row = jnp.clip(wanted_ref[reader, rank], 0, held - 1)
            out_refs[j][rank] = made_ref[row]


def tokens_kernel(
    after_ref,
    scale_ref,
    tok_ref,
    wq_ref,
    wk_ref,
    wd_ref,
    wv_ref,
    wr_ref,
    wg_ref,
    rate_ref,
    qgain_ref,
    gla_ref,
    gate_ref,
    rq_ref,
    narrow_ref,
    wide_ref,
    state_ref,
):
    step = pl.program_id(0)

    @pl.when(step == 0)
    def _():
        state_ref[...] = jnp.zeros_like(state_ref)
        narrow_ref[:DK] = wq_ref[...]
        narrow_ref[DK : 2 * DK] = wk_ref[...]
        narrow_ref[2 * DK :] = wd_ref[...]
        wide_ref[:, :DV] = wv_ref[...]
        wide_ref[:, DV:] = wr_ref[...]

    tokens = tok_ref[...]
    blocks = tokens.shape[0] // BLK
    narrow = nt(tokens, narrow_ref[...])
    wide = jnp.dot(tokens, wide_ref[...], preferred_element_type=F32)
    gate_ref[...] = jax.nn.sigmoid(jnp.dot(tokens, wg_ref[...], preferred_element_type=F32))
    rq_ref[...] = head_norm(wide[:, DV:], qgain_ref[...]).astype(BF16)
    row_id = lax.broadcasted_iota(jnp.int32, (BLK, BLK), 0)
    col_id = lax.broadcasted_iota(jnp.int32, (BLK, BLK), 1)
    causal = row_id >= col_id
    lower = causal.astype(F32)
    places = [slice(b * BLK, (b + 1) * BLK) for b in range(blocks)]
    totals = []
    for b, at in enumerate(places):
        log_decay = -2.0 * rate_ref[...] * jax.nn.sigmoid(narrow[at, 2 * DK :]) * scale_ref[step * blocks + b]
        totals.append(jnp.dot(lower, log_decay, precision=PRECISE, preferred_element_type=F32))
    parts = []
    for at, total in zip(places, totals):
        key = narrow[at, DK : 2 * DK]
        q_dec = narrow[at, :DK] * DK ** (-0.5) * jnp.exp(total)
        k_dec = key * jnp.exp(-total)
        scores = jnp.where(causal, nt(q_dec, k_dec, PRECISE), 0.0)
        parts.append((q_dec, scores, key * jnp.exp(total[BLK - 1 :] - total)))
    inner = []
    for at, (_, scores, k_end) in zip(places, parts):
        value = wide[at, :DV]
        within = jnp.dot(scores, value, precision=PRECISE, preferred_element_type=F32)
        update = lax.dot_general(
            value, k_end, (((0,), (0,)), ((), ())), precision=PRECISE, preferred_element_type=F32
        )
        inner.append((within, update))
    for at, total, (q_dec, _, _), (within, update) in zip(places, totals, parts, inner):
        gla_ref[at] = within + nt(q_dec, state_ref[...], PRECISE)
        state_ref[...] = state_ref[...] * jnp.exp(total[BLK - 1 :]) + update


def add_reads(offsets, st_size, block_ref, rq_ref, got_refs, top_ref, bottom_ref):
    ones = jnp.ones((PLEN, DV), BF16)
    blocks = rq_ref.shape[0]
    me = lax.axis_index("st")
    items = []
    for j, (step, flip) in enumerate(offsets):
        owner = other_index(me, st_size, step, flip, -1)
        for rank in range(block_ref.shape[1]):
            items.append((got_refs[j], rank, jnp.clip(block_ref[owner, rank], 0, blocks - 1)))
    for first in range(0, len(items), GROUP):
        group = items[first : first + GROUP]
        scores = [nt(rq_ref[b], ref[rank, :, :DV]) for ref, rank, b in group]
        weights = [jnp.exp(score * DV ** (-0.5)).astype(BF16) for score in scores]
        reads = [
            jnp.dot(weight, ref[rank, :, DV:], preferred_element_type=F32)
            for weight, (ref, rank, _) in zip(weights, group)
        ]
        sums = [jnp.dot(weight, ones, preferred_element_type=F32) for weight in weights]
        for row_sum, read, (_, _, b) in zip(sums, reads, group):
            bottom_ref[b] += row_sum
            top_ref[b] += read


def early_kernel(offsets, st_size, block_ref, rq_ref, *refs):
    got_refs, (top_ref, bottom_ref) = refs[:-2], refs[-2:]
    top_ref[...] = jnp.zeros_like(top_ref)
    bottom_ref[...] = jnp.zeros_like(bottom_ref)
    add_reads(offsets, st_size, block_ref, rq_ref, got_refs, top_ref, bottom_ref)


def middle_kernel(offsets, st_size, block_ref, rq_ref, top_in_ref, bottom_in_ref, *refs):
    got_refs, (top_ref, bottom_ref) = refs[:-2], refs[-2:]
    top_ref[...] = top_in_ref[...]
    bottom_ref[...] = bottom_in_ref[...]
    add_reads(offsets, st_size, block_ref, rq_ref, got_refs, top_ref, bottom_ref)


def late_kernel(offsets, st_size, block_ref, rq_ref, gla_ref, gate_ref, top_in_ref, bottom_in_ref, *refs):
    got_refs = refs[: len(offsets)]
    out_ref, square_ref, top_ref, bottom_ref = refs[len(offsets) :]
    top_ref[...] = top_in_ref[...]
    bottom_ref[...] = bottom_in_ref[...]
    add_reads(offsets, st_size, block_ref, rq_ref, got_refs, top_ref, bottom_ref)
    blocks = rq_ref.shape[0]
    lane = lax.broadcasted_iota(jnp.int32, (BLK, DV), 1)
    sums = jnp.zeros((BLK, DV), F32)
    for b in range(blocks):
        combined = gla_ref[b] + gate_ref[b] * (top_ref[b] / bottom_ref[b])
        out_ref[b] = combined
        sums = jnp.where(lane == b, jnp.sum(combined * combined, axis=-1, keepdims=True), sums)
    rows = jnp.transpose(sums)[:blocks].reshape(1, blocks, 1, BLK)
    square_ref[...] = jnp.broadcast_to(rows, square_ref.shape)


def scale_kernel(square_ref, combined_ref, gain_ref, out_ref):
    total = jnp.sum(square_ref[...], axis=0)[:, 0, :]
    scale = lax.rsqrt(total / (HEADS * DV) + EPS)
    columns = jnp.transpose(scale)
    for b in range(total.shape[0]):
        at = slice(b * BLK, (b + 1) * BLK)
        out_ref[at] = (combined_ref[at] * columns[:, b : b + 1] * gain_ref[...]).astype(BF16)


VMEM = pl.BlockSpec(memory_space=pltpu.VMEM)
SMEM = pl.BlockSpec(memory_space=pltpu.SMEM)
ANY = pl.BlockSpec(memory_space=pl.ANY)


def whole(shape):
    return pl.BlockSpec(shape, lambda i: (0,) * len(shape))


def on_device(
    tokens,
    w_query,
    w_key,
    w_value,
    w_decay,
    decay_rate,
    block_scale,
    w_rquery,
    w_gate,
    w_rkey,
    w_rvalue,
    query_gain,
    key_gain,
    out_gain,
    store,
    passage_ids,
):
    length, width = tokens.shape
    blocks = length // BLK
    held, plen, _ = store.shape
    st_size = lax.axis_size("st")
    tp_size = lax.axis_size("tp")
    requests = passage_ids.shape[0] * passage_ids.shape[1]
    owners = min(st_size, requests // 2)
    most = requests // owners
    chips = st_size // 2

    wanted, block_of = pl.pallas_call(
        functools.partial(requests_kernel, held),
        out_shape=(
            jax.ShapeDtypeStruct((st_size, most), jnp.int32),
            jax.ShapeDtypeStruct((st_size, most), jnp.int32),
        ),
        in_specs=[VMEM],
        out_specs=(VMEM, VMEM),
        cost_estimate=pl.CostEstimate(flops=64 * held * plen * width * DV, bytes_accessed=0, transcendentals=0),
        compiler_params=pltpu.CompilerParams(vmem_limit_bytes=2 * MIB),
        name="requests",
    )(passage_ids.T)
    incoming = lax.all_to_all(wanted, "st", split_axis=0, concat_axis=0, tiled=True)

    made = pl.pallas_call(
        passages_kernel,
        out_shape=jax.ShapeDtypeStruct((held, plen, 2 * DV), BF16),
        in_specs=[VMEM, VMEM, VMEM, VMEM],
        out_specs=VMEM,
        scratch_shapes=[pltpu.VMEM((width, 2 * DV), BF16)],
        cost_estimate=pl.CostEstimate(
            flops=2 * held * plen * width * 2 * DV,
            bytes_accessed=2 * held * plen * (width + 2 * DV),
            transcendentals=0,
        ),
        compiler_params=pltpu.CompilerParams(vmem_limit_bytes=24 * MIB),
        name="passages",
    )(store, w_rkey, w_rvalue, key_gain.reshape(1, DV))

    half = chips // 2
    order = []
    for step in [*range(2, half + 1), 1]:
        ways = tuple(dict.fromkeys((step, chips - step)))
        order += [(way, flip) for flip in (0, 1) for way in ways]
    near = [o for o in order if min(o[0], chips - o[0]) == 1]
    lead = [o for o in near if o[1] == 0]
    order = lead + [o for o in order if o not in lead]
    offsets = tuple(order + [(0, 1), (0, 0)])
    packed = pl.pallas_call(
        functools.partial(pack_kernel, offsets, st_size),
        out_shape=tuple(jax.ShapeDtypeStruct((most, plen, 2 * DV), BF16) for _ in offsets),
        in_specs=[SMEM, VMEM],
        out_specs=tuple(VMEM for _ in offsets),
        compiler_params=pltpu.CompilerParams(vmem_limit_bytes=8 * MIB),
        name="pack",
    )(incoming, made)

    def sent(array, step, flip):
        pairs = [
            (2 * y + e, ((y + (step, -step)[e]) % chips) * 2 + (e + flip) % 2) for y in range(chips) for e in range(2)
        ]
        return lax.ppermute(array, "st", pairs)

    got = [packed[j] if o == (0, 0) else sent(packed[j], *o) for j, o in enumerate(offsets)]

    rows = 4 * BLK
    gla, gate, read_query = pl.pallas_call(
        tokens_kernel,
        grid=(length // rows,),
        out_shape=(
            jax.ShapeDtypeStruct((length, DV), F32),
            jax.ShapeDtypeStruct((length, DV), F32),
            jax.ShapeDtypeStruct((length, DV), BF16),
        ),
        in_specs=[
            ANY,
            SMEM,
            pl.BlockSpec((rows, width), lambda i: (i, 0)),
            whole((DK, width)),
            whole((DK, width)),
            whole((DK, width)),
            whole((width, DV)),
            whole((width, DV)),
            whole((width, DV)),
            whole((1, DK)),
            whole((1, DV)),
        ],
        out_specs=(
            pl.BlockSpec((rows, DV), lambda i: (i, 0)),
            pl.BlockSpec((rows, DV), lambda i: (i, 0)),
            pl.BlockSpec((rows, DV), lambda i: (i, 0)),
        ),
        scratch_shapes=[
            pltpu.VMEM((3 * DK, width), BF16),
            pltpu.VMEM((width, 2 * DV), BF16),
            pltpu.VMEM((DV, DK), F32),
        ],
        cost_estimate=pl.CostEstimate(
            flops=20 * length * width * (3 * DK + 3 * DV), bytes_accessed=2 * length * width, transcendentals=0
        ),
        compiler_params=pltpu.CompilerParams(vmem_limit_bytes=51 * MIB),
        name="tokens",
    )(
        packed[-1],
        block_scale,
        tokens,
        w_query.T,
        w_key.T,
        w_decay.T,
        w_value,
        w_rquery,
        w_gate,
        decay_rate.reshape(1, DK),
        query_gain.reshape(1, DV),
    )

    blocked = (blocks, BLK, DV)
    read_query = read_query.reshape(blocked)
    sums = jax.ShapeDtypeStruct(blocked, F32)
    last = [j for j, o in enumerate(offsets) if o in near and o not in lead]
    middle = [j for j, (step, _) in enumerate(offsets) if step == half]
    first = [j for j in range(len(offsets)) if j not in last + middle]
    top, bottom = pl.pallas_call(
        functools.partial(early_kernel, tuple(offsets[j] for j in first), st_size),
        out_shape=(sums, sums),
        in_specs=[SMEM, VMEM] + [VMEM] * len(first),
        out_specs=(VMEM, VMEM),
        cost_estimate=pl.CostEstimate(
            flops=8 * len(first) * most * BLK * plen * DV, bytes_accessed=0, transcendentals=0
        ),
        compiler_params=pltpu.CompilerParams(vmem_limit_bytes=14 * MIB),
        name="early",
    )(block_of, read_query, *[got[j] for j in first])
    top, bottom = pl.pallas_call(
        functools.partial(middle_kernel, tuple(offsets[j] for j in middle), st_size),
        out_shape=(sums, sums),
        in_specs=[SMEM] + [VMEM] * (3 + len(middle)),
        out_specs=(VMEM, VMEM),
        cost_estimate=pl.CostEstimate(
            flops=8 * len(middle) * most * BLK * plen * DV, bytes_accessed=0, transcendentals=0
        ),
        compiler_params=pltpu.CompilerParams(vmem_limit_bytes=14 * MIB),
        name="middle",
    )(block_of, read_query, top, bottom, *[got[j] for j in middle])
    combined, squares = pl.pallas_call(
        functools.partial(late_kernel, tuple(offsets[j] for j in last), st_size),
        out_shape=(sums, jax.ShapeDtypeStruct((tp_size, blocks, 1, BLK), F32)),
        in_specs=[SMEM] + [VMEM] * (5 + len(last)),
        out_specs=(VMEM, VMEM),
        scratch_shapes=[pltpu.VMEM(blocked, F32), pltpu.VMEM(blocked, F32)],
        compiler_params=pltpu.CompilerParams(vmem_limit_bytes=14 * MIB),
        name="late",
    )(
        block_of,
        read_query,
        gla.reshape(blocked),
        gate.reshape(blocked),
        top,
        bottom,
        *[got[j] for j in last],
    )
    everyone = lax.all_to_all(squares, "tp", split_axis=0, concat_axis=0, tiled=True)

    return pl.pallas_call(
        scale_kernel,
        out_shape=jax.ShapeDtypeStruct((length, DV), BF16),
        in_specs=[VMEM, VMEM, VMEM],
        out_specs=VMEM,
        compiler_params=pltpu.CompilerParams(vmem_limit_bytes=8 * MIB),
        name="scale",
    )(everyone, combined.reshape(length, DV), out_gain.reshape(1, DV))


def solution(mesh):
    return jax.shard_map(
        on_device,
        mesh=mesh,
        in_specs=(
            P(("grp", "st"), None),
            P(None, "tp"),
            P(None, "tp"),
            P(None, "tp"),
            P(None, "tp"),
            P("tp"),
            P(("grp", "st")),
            P(None, "tp"),
            P(None, "tp"),
            P(None, "tp"),
            P(None, "tp"),
            P(),
            P(),
            P("tp"),
            P(("grp", "st"), None, None),
            P(("grp", "st"), None),
        ),
        out_specs=P(("grp", "st"), "tp"),
        check_vma=False,
    )
```
